256 devices in a mesh: sp: 64 (over z, y, core), tp: 4 (over x).
Axes of the slice: x: 4, y: 4, z: 8, core: 2. Of those that a mesh axis runs over, the one named last changes fastest.
Arguments:
- queries: bfloat16 [32768, 1024], P('sp', 'tp'), may hold values from -160 to 160
- keys: bfloat16 [32768, 256], P('sp', 'tp'), may hold values from -5 to 5
- values: bfloat16 [32768, 256], P('sp', 'tp'), may hold values from -6 to 6
- doc_ids: int32 [32768], P('sp'), may hold values from 0 to 31, never falling along the last dimension, each value on 1 to 2048 neighbouring positions
- sink_logit: float32 [16], P('tp'), may hold values from 1 to 6
- w_out: bfloat16 [1024, 2048], P('tp'), may hold values from -0.1875 to 0.1875
- residual: bfloat16 [32768, 2048], P(('sp', 'tp')), may hold values from -6 to 6
- ffn_gain: float32 [2048], replicated, may hold values from 0.1 to 1.9
- expert_ids: int32 [32768, 8], P(('sp', 'tp')), may hold values from 0 to 63, all different within a row; in each aligned block of 64 rows (0 to 63, 64 to 127, ...) at most 12 rows name the same one
- expert_weight: float32 [32768, 8], P(('sp', 'tp')), may hold values from 0.2 to 2
- exp_gate: bfloat16 [64, 2048, 512], P('sp'), may hold values from -0.125 to 0.125
- exp_up: bfloat16 [64, 2048, 512], P('sp'), may hold values from -0.125 to 0.125
- exp_down: bfloat16 [64, 512, 2048], P('sp'), may hold values from -0.25 to 0.25
- shared_gate: bfloat16 [2048, 512], P(None, 'tp'), may hold values from -0.125 to 0.125
- shared_up: bfloat16 [2048, 512], P(None, 'tp'), may hold values from -0.125 to 0.125
- shared_down: bfloat16 [512, 2048], P('tp'), may hold values from -0.25 to 0.25
Outputs:
- output: bfloat16 [32768, 2048], P(('sp', 'tp'))
The draws below stay inside these ranges and needn't reach their ends.
Inputs may be any that keep to these rules, and one draw needn't show every extreme that they name: `doc_ids`: never falling along the sequence; every document holds at most 2048 positions, and one holds exactly that many. `expert_ids`: each row names 8 different experts. In each aligned block of 64 rows no expert is named by more than 12 rows, and in some blocks one expert is named by exactly 12 rows.
All inputs are finite; a program needn't handle non-finite values.
Results may differ from the reference program's by a relative error of at most 0.018.
Values may be sent and summed in bfloat16 or wider, within the bound.
A program may use at most 128 MiB of HBM per device.

```python
import math
import jax
import jax.numpy as jnp
import numpy as np
from jax import lax

D = 2048
HQ = 16
KV = 4
HD = 64
WINDOW = 128
FF = 512
SFF = 512
TOP_K = 8
TOK_DEV = 512
ATTN_W = 1024
TOKENS = 32768
HALF = 64
EXPERTS = 64
CAP = 12
DOCS = 32
N_TP = 4


def drawn_pair(key):
    base_keys = jnp.clip(jax.random.normal(jax.random.fold_in(key, 101), (TOKENS, KV, HD), jnp.float32), -5.0, 5.0)
    return base_keys


def draw_keys(key, part):
    base_keys = drawn_pair(key)
    result = base_keys
    return result.reshape(TOKENS, KV * HD).astype(jnp.bfloat16)


def draw_queries(key, part):
    drawn_rows = jnp.clip(jax.random.normal(jax.random.fold_in(key, 105), (TOKENS, HQ * HD), jnp.float32), -5.0, 5.0)
    result = drawn_rows
    return result.astype(jnp.bfloat16)


def block_scale(stream_key, extent, cuts, smallest, high):
    factor_of, own = 1.0, jax.random.fold_in(stream_key, 6)
    for axis_at, parts in cuts:
        heights = jnp.exp(jax.random.uniform(jax.random.fold_in(own, axis_at), (parts,), jnp.float32, smallest / len(cuts), high / len(cuts)))
        factor_of = factor_of * jnp.repeat(heights, extent[axis_at] // parts).reshape([-1 if axis == axis_at else 1 for axis in range(len(extent))])
    return factor_of


def split_up(count, total, bound, lean):
    loads = [(1 << 20) // math.isqrt(rank ** lean) + 1 for rank in range(2, count + 1)]
    rest, given = total - bound - (count - 1), [1] * (count - 1)
    while rest > 0:
        free = [i for i in range(count - 1) if given[i] < bound]
        whole, budget = sum([loads[i] for i in free]), rest
        for i in free:
            extra = min(bound - given[i], max(1, budget * loads[i] // whole), rest)
            given[i] = given[i] + extra
            rest = rest - extra
    return np.array([bound] + given)


def uneven_parts(rng, count, total, limit, lean):
    if count == 2:
        one = jax.random.randint(rng, (), max(1, total - limit), min(limit, total - 1) + 1)
        return jnp.stack([one, total - one])
    lengths = jnp.asarray(split_up(count, total, limit, lean), jnp.int32)
    pairs = (count - 1) // 2
    source_of, receiver = lengths[1:1 + 2 * pairs:2], lengths[2:2 + 2 * pairs:2]
    slack = jnp.minimum(source_of - 1, limit - receiver)
    moved = jax.random.randint(jax.random.fold_in(rng, 1), (pairs,), 0, 1 << 20) % (slack + 1)
    lengths = lengths.at[1:1 + 2 * pairs:2].set(source_of - moved).at[2:2 + 2 * pairs:2].set(receiver + moved)
    return lengths[jax.random.permutation(jax.random.fold_in(rng, 2), count)]


def routed_block(key, own, number, rows, number_of, top, bound, lean):
    ranking = jax.random.permutation(key, number_of)
    packed, common = shares(number_of, rows * top, bound, lean, True), shares(number_of, rows * top, bound, lean, False)
    places = jnp.arange(number_of)

    def named(sizes, turn):
        used = int((sizes > 0).sum())
        fixed = max(1, used // 4)
        passed = fixed + (places - fixed + turn * (used - fixed)) % max(1, number_of - fixed)
        return jnp.zeros((number_of,), jnp.int32).at[ranking[jnp.where(places < fixed, places, passed)]].set(jnp.asarray(sizes, jnp.int32))

    sizes = jnp.where(number % 4 == 0, named(packed, number // 4), named(common, number - number // 4 - 1))
    mixed = jax.random.permutation(jax.random.fold_in(own, 3), number_of)
    donor, sink = mixed[0:number_of // 2 * 2:2], mixed[1:number_of // 2 * 2:2]
    room = jnp.minimum(sizes[donor] - 1, bound - sizes[sink]) // 2
    room = jnp.where((donor == ranking[0]) | (sink == ranking[0]) | (sizes[sink] == 0), 0, jnp.maximum(room, 0))
    passed = jax.random.randint(jax.random.fold_in(own, 4), (number_of // 2,), 0, 1 << 20) % (room + 1)
    sizes = sizes.at[donor].add(-passed).at[sink].add(passed)
    members = jnp.searchsorted(jnp.cumsum(sizes), jnp.arange(rows * top), side="right").astype(jnp.int32)
    listing = members.reshape(top, rows).T
    listing = listing[jax.random.permutation(jax.random.fold_in(own, 1), rows)]
    turn = jax.random.randint(jax.random.fold_in(own, 2), (rows, 1), 0, top)
    return jnp.take_along_axis(listing, (jnp.arange(top)[None, :] + turn) % top, axis=1)


def shares(amount, total, reach, skew, full):
    weights = [(1 << 20) // math.isqrt(grade ** skew) + 1 for grade in range(1, amount + 1)]
    largest = reach if full else min(reach, max(-(-total // amount), total * weights[0] // sum(weights)))
    least = 1 if total - largest >= amount - 1 else 0
    given, surplus = [largest] + [least] * (amount - 1), total - largest - least * (amount - 1)
    while surplus > 0:
        candidates = [i for i in range(1, amount) if given[i] < largest] or [i for i in range(1, amount) if given[i] < reach]
        pool, budget = sum([weights[i] for i in candidates]), surplus
        for i in candidates:
            more = min(reach - given[i], max(1, budget * weights[i] // pool), surplus)
            given[i] = given[i] + more
            surplus = surplus - more
    return np.array(given)


def centred(key, extent, deviation, limit, shards=(), kind=jnp.bfloat16):
    values = deviation * jax.random.normal(key, extent, jnp.float32)
    if shards:
        values = values * block_scale(key, extent, shards, -0.22, 0.18)
    return jnp.clip(values, -limit, limit).astype(kind)


def setup_inputs(seed: int = 0) -> dict:
    splits = jax.random.split(jax.random.key(seed), 17)
    queries = draw_queries(jax.random.fold_in(splits[16], 71), 0)
    keys = draw_keys(jax.random.fold_in(splits[16], 71), 0)
    values = centred(splits[2], (TOKENS, KV * HD), 1.0, 6.0, ((0, 64), (1, 4)))
    doc_ids = jnp.searchsorted(jnp.cumsum(uneven_parts(splits[3], DOCS, TOKENS, 4 * TOK_DEV, 2)), jnp.arange(TOKENS), side="right").astype(jnp.int32)
    sink_logit = jnp.clip(1.0 + 5.0 * jax.random.uniform(splits[4], (HQ,), jnp.float32) ** block_scale(splits[4], (HQ,), ((0, 4),), -0.2, 0.2), 1.0, 6.0)
    w_out = centred(splits[5], (ATTN_W, D), ATTN_W ** -0.5, 0.1875, ((0, 4),))
    residual = centred(splits[6], (TOKENS, D), 1.0, 6.0, ((0, 256),))
    ffn_gain = jnp.clip(1.0 + 0.18 * jax.random.normal(splits[7], (D,), jnp.float32), 0.1, 1.9)
    expert_ids_keys = jax.random.split(jax.random.fold_in(splits[8], 1), TOKENS // HALF)
    expert_ids_turns = jax.random.permutation(jax.random.fold_in(splits[8], 3), TOKENS // HALF)
    expert_ids = jax.vmap(lambda own, number: routed_block(jax.random.fold_in(splits[8], 2), own, number, HALF, EXPERTS, TOP_K, CAP, 2))(expert_ids_keys, expert_ids_turns).reshape((TOKENS, TOP_K))
    expert_weight = jnp.clip(jnp.exp(math.log(2.0) - 2.3025851 * jax.random.uniform(splits[9], (TOKENS, TOP_K), jnp.float32) ** block_scale(splits[9], (TOKENS, TOP_K), ((0, 256),), -0.2, 0.2)), 0.2, 2.0)
    exp_gate = centred(splits[10], (EXPERTS, D, FF), D ** -0.5, 0.125, ((0, 64),))
    exp_up = centred(splits[11], (EXPERTS, D, FF), D ** -0.5, 0.125, ((0, 64),))
    exp_down = centred(splits[12], (EXPERTS, FF, D), FF ** -0.5, 0.25, ((0, 64),))
    shared_gate = centred(splits[13], (D, SFF), D ** -0.5, 0.125, ((1, 4),))
    shared_up = centred(splits[14], (D, SFF), D ** -0.5, 0.125, ((1, 4),))
    shared_down = centred(splits[15], (SFF, D), SFF ** -0.5, 0.25, ((0, 4),))
    return dict(queries=queries, keys=keys, values=values, doc_ids=doc_ids, sink_logit=sink_logit, w_out=w_out, residual=residual, ffn_gain=ffn_gain, expert_ids=expert_ids, expert_weight=expert_weight, exp_gate=exp_gate, exp_up=exp_up, exp_down=exp_down, shared_gate=shared_gate, shared_up=shared_up, shared_down=shared_down)


norm_eps = 1e-06

def band_blocks(padded, width):
    span_count = padded.shape[0] // width - 2
    shaped = padded.reshape((span_count + 2, width) + padded.shape[1:])
    return jnp.concatenate([shaped[0:span_count:2], shaped[1:span_count + 1:2], shaped[2:span_count + 2:2], shaped[3:span_count + 3:2]], axis=1)

def reference(queries, keys, values, doc_ids, sink_logit, w_out, residual, ffn_gain, expert_ids, expert_weight, exp_gate, exp_up, exp_down, shared_gate, shared_up, shared_down):
    group_size = HQ // KV
    query_span = 2 * WINDOW
    block_count = TOKENS // query_span
    pad_rows = ((WINDOW, WINDOW), (0, 0))
    key_blocks = band_blocks(jnp.pad(keys, pad_rows), WINDOW).reshape(block_count, 4 * WINDOW, KV, HD)
    value_blocks = band_blocks(jnp.pad(values, pad_rows), WINDOW).reshape(block_count, 4 * WINDOW, KV, HD)
    marks = (doc_ids + 1).astype(jnp.int32)
    mark_blocks = band_blocks(jnp.pad(marks, (WINDOW, WINDOW)), WINDOW)
    query_blocks = queries.reshape(block_count, query_span, KV, group_size, HD)
    query_marks = marks.reshape(block_count, query_span)
    offset = jnp.arange(query_span, dtype=jnp.int32)[:, None] - jnp.arange(4 * WINDOW, dtype=jnp.int32)[None, :] + WINDOW
    near = jnp.abs(offset) <= WINDOW
    sink_term = sink_logit.astype(jnp.float32).reshape(KV, group_size)[:, :, None, None]

    def attend_block(inputs):
        query_in, key_in, value_in, key_marks, row_marks = inputs
        scores = jnp.einsum('qkgd,mkd->kgqm', query_in.astype(jnp.float32), key_in.astype(jnp.float32)) * HD ** (-0.5)
        allowed = near & (key_marks[None, :] == row_marks[:, None])
        scores = jnp.where(allowed[None, None], scores, -jnp.inf)
        row_max = jnp.maximum(lax.optimization_barrier(jnp.max(scores, axis=-1, keepdims=True)), sink_term)
        exp_scores = jnp.exp(scores - row_max)
        attn_probs = (exp_scores / (lax.optimization_barrier(jnp.sum(exp_scores, axis=-1, keepdims=True)) + jnp.exp(sink_term - row_max))).astype(jnp.bfloat16)
        result = jnp.einsum('kgqm,mkd->qkgd', attn_probs.astype(jnp.float32), value_in.astype(jnp.float32))
        return result.astype(jnp.bfloat16).reshape(query_span, HQ * HD)
    attended = lax.map(attend_block, (query_blocks, key_blocks, value_blocks, mark_blocks, query_marks)).reshape(TOKENS, HQ * HD)
    mixed = jnp.dot(attended, w_out, preferred_element_type=jnp.float32)
    resid = (residual.astype(jnp.float32) + mixed).astype(jnp.bfloat16)
    resid_f = resid.astype(jnp.float32)
    normed = (resid_f * lax.rsqrt(lax.optimization_barrier(jnp.mean(resid_f * resid_f, axis=-1, keepdims=True)) + norm_eps) * ffn_gain.astype(jnp.float32)).astype(jnp.bfloat16)
    shared_hidden = (jax.nn.silu(jnp.dot(normed, shared_gate, preferred_element_type=jnp.float32)) * jnp.dot(normed, shared_up, preferred_element_type=jnp.float32)).astype(jnp.bfloat16)
    block_units = SFF // N_TP
    shared_out = jnp.zeros((TOKENS, D), jnp.float32)
    for unit_block in range(N_TP):
        lower = unit_block * block_units
        partial_out = jnp.dot(shared_hidden[:, lower:lower + block_units], shared_down[lower:lower + block_units], preferred_element_type=jnp.float32)
        shared_out = shared_out + lax.optimization_barrier(partial_out.astype(jnp.bfloat16)).astype(jnp.float32)
    assign_count = TOKENS * TOP_K
    row_block = 512
    flat_ids = expert_ids.reshape(assign_count).astype(jnp.int32)
    order = jnp.argsort(flat_ids, stable=True).astype(jnp.int32)
    sorted_ids = flat_ids[order]
    counts = jnp.bincount(flat_ids, length=EXPERTS).astype(jnp.int32)
    starts = (jnp.cumsum(counts) - counts).astype(jnp.int32)
    padded = ((counts + row_block - 1) // row_block * row_block).astype(jnp.int32)
    ends = jnp.cumsum(padded).astype(jnp.int32)
    pad_starts = (ends - padded).astype(jnp.int32)
    dest = (pad_starts[sorted_ids] + jnp.arange(assign_count, dtype=jnp.int32) - starts[sorted_ids]).astype(jnp.int32)
    block_total = -(-assign_count // row_block) + EXPERTS
    row_source = jnp.full((block_total * row_block,), assign_count, jnp.int32).at[dest].set(order)
    block_expert = jnp.minimum(jnp.searchsorted(ends, jnp.arange(block_total, dtype=jnp.int32) * row_block, side='right'), EXPERTS - 1).astype(jnp.int32)
    flat_weight = expert_weight.reshape(assign_count).astype(jnp.float32)

    def expert_step(running, inputs):
        sources, expert_index = inputs
        live = sources < assign_count
        safe = jnp.minimum(sources, assign_count - 1)
        token_rows = (safe // TOP_K).astype(jnp.int32)
        gathered = normed[token_rows]
        hidden = (jax.nn.silu(jnp.dot(gathered, exp_gate[expert_index], preferred_element_type=jnp.float32)) * jnp.dot(gathered, exp_up[expert_index], preferred_element_type=jnp.float32)).astype(jnp.bfloat16)
        produced = jnp.dot(hidden, exp_down[expert_index], preferred_element_type=jnp.float32).astype(jnp.bfloat16)
        scale = jnp.where(live, flat_weight[safe], jnp.zeros_like(flat_weight[safe]))
        return (running.at[token_rows].add(scale[:, None] * produced.astype(jnp.float32)), None)
    routed, _ = lax.scan(expert_step, jnp.zeros((TOKENS, D), jnp.float32), (row_source.reshape(block_total, row_block), block_expert))
    return (resid.astype(jnp.float32) + shared_out + routed).astype(jnp.bfloat16)
```

```python
import functools

import jax
import jax.numpy as jnp
from jax import lax
from jax.experimental import pallas as pl
from jax.experimental.pallas import tpu as pltpu
from jax.sharding import PartitionSpec as P

HD = 64
WINDOW = 128
NZ, NY, NC, NX = 8, 4, 2, 4
PLANE = NY * NC
ROWS = 128
HALF = 64
CAP = 12
SLOTS = 2 * CAP
PACK = PLANE * SLOTS
D = 2048
FF = 512
EXPERTS = 64
MESH = pl.DeviceIdType.MESH
BF = jnp.bfloat16
F32 = jnp.float32

norm_eps = 1e-06


def extended(cells, sides, width):
    for axis, dim in sides:
        count = lax.axis_size(axis)
        ends = count - 1
        head = lax.slice_in_dim(cells, 0, width, axis=dim)
        tail = lax.slice_in_dim(cells, cells.shape[dim] - width, cells.shape[dim], axis=dim)
        cells = jnp.concatenate(
            [
                lax.ppermute(tail, axis, [(i, (i + 1) % count) for i in range(ends)]),
                cells,
                lax.ppermute(head, axis, [((i + 1) % count, i) for i in range(ends)]),
            ],
            axis=dim,
        )
    return cells


def band_blocks(padded, width):
    span_count = padded.shape[0] // width - 2
    shaped = padded.reshape((span_count + 2, width) + padded.shape[1:])
    return jnp.concatenate(
        [
            shaped[0:span_count:2],
            shaped[1 : span_count + 1 : 2],
            shaped[2 : span_count + 2 : 2],
            shaped[3 : span_count + 3 : 2],
        ],
        axis=1,
    )


def attend(queries, ext_keys, ext_values, ext_marks, own_marks, sink_logit):
    tok_count = queries.shape[0]
    head_count = sink_logit.shape[0]
    key_heads = ext_keys.shape[1] // HD
    group_size = head_count // key_heads
    query_span = 2 * WINDOW
    block_count = tok_count // query_span
    query_blocks = queries.reshape(block_count, query_span, key_heads, group_size, HD)
    key_blocks = band_blocks(ext_keys, WINDOW).reshape(block_count, 4 * WINDOW, key_heads, HD)
    value_blocks = band_blocks(ext_values, WINDOW).reshape(block_count, 4 * WINDOW, key_heads, HD)
    mark_blocks = band_blocks(ext_marks, WINDOW)
    query_marks = own_marks.reshape(block_count, query_span)
    scores = jnp.einsum(
        "nqkgd,nmkd->nkgqm", query_blocks, key_blocks, preferred_element_type=jnp.float32
    ) * HD ** (-0.5)
    offset = (
        jnp.arange(query_span, dtype=jnp.int32)[:, None]
        - jnp.arange(4 * WINDOW, dtype=jnp.int32)[None, :]
        + WINDOW
    )
    allowed = (jnp.abs(offset) <= WINDOW)[None] & (
        mark_blocks[:, None, :] == query_marks[:, :, None]
    )
    scores = jnp.where(allowed[:, None, None], scores, -jnp.inf)
    sink_term = sink_logit.reshape(key_heads, group_size)[None, :, :, None, None]
    row_max = jnp.maximum(jnp.max(scores, axis=-1, keepdims=True), sink_term)
    exp_scores = jnp.exp(scores - row_max)
    attn_probs = (
        exp_scores / (jnp.sum(exp_scores, axis=-1, keepdims=True) + jnp.exp(sink_term - row_max))
    ).astype(jnp.bfloat16)
    result = jnp.einsum(
        "nkgqm,nmkd->nqkgd", attn_probs, value_blocks, preferred_element_type=jnp.float32
    )
    return result.astype(jnp.bfloat16).reshape(tok_count, head_count * HD)


def dot(a, b):
    return jnp.dot(a, b, preferred_element_type=F32)


def silu(v):
    return v / (1.0 + jnp.exp(-v))


def chunk_of(delta):
    return 0 if delta == 0 else (2 * delta - 1 if delta <= NZ // 2 else 2 * (NZ - delta))


def moe_kernel(
    normed, resid, ids, weight, eg, eu, ed, shg, shu, shd, out,
    tok, tx, rx, eo, ret, rst, rsx, info, inf, wg, wu, wd, sg, su, sd, sacc, hid,
    z_s, z_r, i_s, i_r, d_s, d_r, e_s, e_r, p_s, p_r, x_s, x_r, w_s,
):
    sp, x = lax.axis_index("sp"), lax.axis_index("tp")
    z, mine = sp // PLANE, sp % PLANE

    def at_z(dz):
        return ((z + dz) % NZ * PLANE + mine, x)

    def at_plane(j):
        return (z * PLANE + j, x)

    def at_x(dx):
        return (sp, (x + dx) % NX)

    def send(src, dst, ssem, rsem, device):
        copy = pltpu.make_async_remote_copy(
            src_ref=src, dst_ref=dst, send_sem=ssem, recv_sem=rsem, device_id=device, device_id_type=MESH
        )
        copy.start()

    def landed(ref, sem):
        pltpu.make_async_copy(ref, ref, sem).wait()

    local = [
        pltpu.make_async_copy(normed, tok.at[0], w_s.at[0]),
        pltpu.make_async_copy(shg, sg.at[0], w_s.at[1]),
        pltpu.make_async_copy(shu, su.at[0], w_s.at[2]),
        pltpu.make_async_copy(shd, sd.at[0], w_s.at[3]),
        pltpu.make_async_copy(eg.at[0], wg, w_s.at[4]),
        pltpu.make_async_copy(eu.at[0], wu, w_s.at[5]),
        pltpu.make_async_copy(ed.at[0], wd, w_s.at[6]),
    ]
    for copy in local:
        copy.start()

    barrier = pltpu.get_barrier_semaphore()
    peers = [at_z(dz) for dz in range(1, NZ)] + [at_x(dx) for dx in range(1, NX)]
    peers += [at_plane((mine + off) % PLANE) for off in range(1, PLANE)]
    for device in peers:
        pl.semaphore_signal(barrier, inc=1, device_id=device, device_id_type=MESH)

    expert = lax.broadcasted_iota(jnp.int32, (EXPERTS, ROWS), 0)
    hits = jnp.zeros((EXPERTS, ROWS), F32)
    wide = jnp.zeros((EXPERTS, ROWS), F32)
    for k in range(ids.shape[0]):
        named = ids[k : k + 1, :] == expert
        hits = hits + named.astype(F32)
        wide = wide + jnp.where(named, weight[k : k + 1, :], 0.0)
    row = lax.broadcasted_iota(jnp.int32, (ROWS, ROWS), 0)
    col = lax.broadcasted_iota(jnp.int32, (ROWS, ROWS), 1)
    earlier = ((row < col) & (row // HALF == col // HALF)).astype(BF)
    rank = dot(hits.astype(BF), earlier)
    half = lax.broadcasted_iota(jnp.int32, (EXPERTS, ROWS), 1) // HALF
    place = jnp.where(hits > 0.0, rank + (half * CAP).astype(F32), -1.0)
    for plane in range(NZ):
        lower = plane * PLANE
        info[plane, 0:PLANE, :] = place[lower : lower + PLANE]
        info[plane, PLANE : 2 * PLANE, :] = wide[lower : lower + PLANE]
    inf[0] = info[z]

    local[0].wait()
    pl.semaphore_wait(barrier, len(peers))
    for delta in range(1, NZ):
        i = chunk_of(delta)
        send(info.at[(z + delta) % NZ], inf.at[i], i_s.at[i], i_r.at[i], at_z(delta))
    send(tok.at[0], tok.at[1], z_s.at[1], z_r.at[1], at_z(1))
    send(tok.at[0], tok.at[2], z_s.at[2], z_r.at[2], at_z(NZ - 1))

    def placed(i):
        slot = lax.broadcasted_iota(jnp.int32, (PLANE, SLOTS, ROWS), 1).astype(F32)
        return (inf[i, 0:PLANE, :][:, None, :] == slot).astype(F32)

    def dispatch(i):
        @pl.when(i > 0)
        def _():
            landed(tok.at[i], z_r.at[i])
            landed(inf.at[i], i_r.at[i])

        @pl.when((i > 0) & (i + 2 < NZ))
        def _():
            way = 1 + (NZ - 2) * ((i + 1) % 2)
            send(tok.at[i], tok.at[i + 2], z_s.at[i + 2], z_r.at[i + 2], at_z(way))

        pick = placed(i).reshape(PACK, ROWS).astype(BF)
        for n in range(D // 512):
            cols = pl.ds(n * 512, 512)
            tx[i, :, :, cols] = dot(pick, tok[i, :, cols]).astype(BF).reshape(PLANE, SLOTS, 512)
        for off in range(1, PLANE):
            j = (mine + off) % PLANE
            send(tx.at[i, j], rx.at[i, mine], d_s.at[i], d_r.at[i], at_plane(j))
        pltpu.make_async_copy(tx.at[i, mine], rx.at[i, mine], d_r.at[i]).start()

    def run_expert(i):
        landed(rx.at[i], d_r.at[i])

        def hidden_tile(n, carry):
            cols = pl.ds(pl.multiple_of(n * 256, 256), 256)
            rows = rx[i].reshape(PACK, D)
            hid[:, cols] = (silu(dot(rows, wg[:, cols])) * dot(rows, wu[:, cols])).astype(BF)
            return carry

        lax.fori_loop(0, FF // 256, hidden_tile, 0)

        def out_tile(n, carry):
            cols = pl.ds(pl.multiple_of(n * 512, 512), 512)
            eo[i, :, :, cols] = dot(hid[...], wd[:, cols]).astype(BF).reshape(PLANE, SLOTS, 512)
            return carry

        lax.fori_loop(0, D // 512, out_tile, 0)

    def give_back(i):
        for off in range(1, PLANE):
            j = (mine + off) % PLANE
            send(eo.at[i, j], ret.at[i, mine], e_s.at[i], e_r.at[i], at_plane(j))
        pltpu.make_async_copy(eo.at[i, mine], ret.at[i, mine], e_r.at[i]).start()

    LAG = 2

    def forward(i, carry):
        @pl.when(i < NZ)
        def _():
            dispatch(i)

        @pl.when(i == 0)
        def _():
            for dx in range(1, NX):
                send(sg.at[0], sg.at[dx], x_s.at[0, dx], x_r.at[0, dx], at_x(dx))
                send(su.at[0], su.at[dx], x_s.at[1, dx], x_r.at[1, dx], at_x(dx))
                send(sd.at[0], sd.at[dx], x_s.at[2, dx], x_r.at[2, dx], at_x(dx))

        @pl.when(i >= LAG)
        def _():
            run_expert(i - LAG)

        @pl.when(i >= NZ - 2 + LAG)
        def _():
            give_back(i - LAG)

        return carry

    for copy in local[1:]:
        copy.wait()
    lax.fori_loop(0, NZ + LAG, forward, 0)

    def backward(n, carry):
        give_back(NZ - 3 - n)
        return carry

    lax.fori_loop(0, NZ - 2, backward, 0)

    for dx in range(1, NX):
        landed(sg.at[dx], x_r.at[0, dx])
        landed(su.at[dx], x_r.at[1, dx])
        landed(sd.at[dx], x_r.at[2, dx])
    sacc[...] = jnp.zeros_like(sacc)

    def shared_block(dx, carry):
        rows = tok[0]
        units = (silu(dot(rows, sg[dx])) * dot(rows, su[dx])).astype(BF)
        for n in range(D // 512):
            cols = pl.ds(n * 512, 512)
            sacc[:, cols] = sacc[:, cols] + dot(units, sd[dx, :, cols])
        return carry

    lax.fori_loop(0, NX, shared_block, 0)

    def combined(i):
        landed(ret.at[i], e_r.at[i])
        scaled = placed(i) * inf[i, PLANE : 2 * PLANE, :][:, None, :]
        scaled = jnp.concatenate([scaled.reshape(PACK, ROWS), jnp.zeros((256 - PACK, ROWS), F32)], axis=0)
        scaled = scaled.T[:, :PACK]
        high = scaled.astype(BF)
        low = (scaled - high.astype(F32)).astype(BF)

        def part(cols):
            rows = ret[i, :, :, cols].reshape(PACK, 512)
            return dot(high, rows) + dot(low, rows)

        return part

    def pass_on(i):
        way = NZ - 1 - (NZ - 2) * ((i + 1) % 2)
        send(rst.at[i], rsx.at[i], p_s.at[i], p_r.at[i], at_z(way))

    def farthest(n, carry):
        i = NZ - 1 - n
        part = combined(i)
        for n in range(D // 512):
            cols = pl.ds(n * 512, 512)
            rst[i, :, cols] = part(cols).astype(BF)
        pass_on(i)
        return carry

    lax.fori_loop(0, 2, farthest, 0)

    def nearer(n, carry):
        i = NZ - 3 - n
        part = combined(i)
        landed(rsx.at[i + 2], p_r.at[i + 2])
        for n in range(D // 512):
            cols = pl.ds(n * 512, 512)
            rst[i, :, cols] = (part(cols) + rsx[i + 2, :, cols].astype(F32)).astype(BF)
        pass_on(i)
        return carry

    lax.fori_loop(0, NZ - 3, nearer, 0)

    part = combined(0)
    landed(rsx.at[2], p_r.at[2])
    landed(rsx.at[1], p_r.at[1])
    for n in range(D // 512):
        cols = pl.ds(n * 512, 512)
        routed = part(cols) + rsx[2, :, cols].astype(F32) + rsx[1, :, cols].astype(F32)
        out[:, cols] = (resid[:, cols].astype(F32) + sacc[:, cols] + routed).astype(BF)

    for i in range(NZ):
        landed(tx.at[i, pl.ds(0, PLANE - 1)], d_s.at[i])
        landed(eo.at[i, pl.ds(0, PLANE - 1)], e_s.at[i])
        if i > 0:
            landed(tok.at[i], z_s.at[i])
            landed(info.at[i], i_s.at[i])
            landed(rst.at[i], p_s.at[i])
    for dx in range(1, NX):
        landed(sg.at[0], x_s.at[0, dx])
        landed(su.at[0], x_s.at[1, dx])
        landed(sd.at[0], x_s.at[2, dx])


def moe(normed, resid, ids, weight, eg, eu, ed, shg, shu, shd):
    vmem = pl.BlockSpec(memory_space=pltpu.VMEM)
    hbm = pl.BlockSpec(memory_space=pl.ANY)
    dma = pltpu.SemaphoreType.DMA
    unit = FF // NX
    return pl.pallas_call(
        moe_kernel,
        out_shape=jax.ShapeDtypeStruct((ROWS, D), BF),
        in_specs=[hbm, vmem, vmem, vmem] + [hbm] * 6,
        out_specs=vmem,
        scratch_shapes=[
            pltpu.VMEM((NZ, ROWS, D), BF),
            pltpu.VMEM((NZ, PLANE, SLOTS, D), BF),
            pltpu.VMEM((NZ, PLANE, SLOTS, D), BF),
            pltpu.VMEM((NZ, PLANE, SLOTS, D), BF),
            pltpu.VMEM((NZ, PLANE, SLOTS, D), BF),
            pltpu.VMEM((NZ, ROWS, D), BF),
            pltpu.VMEM((NZ, ROWS, D), BF),
            pltpu.VMEM((NZ, 2 * PLANE, ROWS), F32),
            pltpu.VMEM((NZ, 2 * PLANE, ROWS), F32),
            pltpu.VMEM((D, FF), BF),
            pltpu.VMEM((D, FF), BF),
            pltpu.VMEM((FF, D), BF),
            pltpu.VMEM((NX, D, unit), BF),
            pltpu.VMEM((NX, D, unit), BF),
            pltpu.VMEM((NX, unit, D), BF),
            pltpu.VMEM((ROWS, D), F32),
            pltpu.VMEM((PACK, FF), BF),
        ]
        + [dma((NZ,))] * 10
        + [dma((3, NX)), dma((3, NX)), dma((7,))],
        compiler_params=pltpu.CompilerParams(
            collective_id=1, has_side_effects=True, vmem_limit_bytes=62 * 2**20
        ),
        name="moe",
    )(normed, resid, ids, weight, eg, eu, ed, shg, shu, shd)


def shards(
    queries,
    keys,
    values,
    doc_ids,
    sink_logit,
    w_out,
    residual,
    ffn_gain,
    expert_ids,
    expert_weight,
    exp_gate,
    exp_up,
    exp_down,
    shared_gate,
    shared_up,
    shared_down,
):
    marks = (doc_ids + 1).astype(jnp.bfloat16)
    ext_keys, ext_values, ext_marks = (
        extended(keys, (("sp", 0),), WINDOW),
        extended(values, (("sp", 0),), WINDOW),
        extended(marks, (("sp", 0),), WINDOW),
    )
    attended = attend(queries, ext_keys, ext_values, ext_marks, marks, sink_logit)
    own_rows = lax.all_to_all(attended, "tp", split_axis=0, concat_axis=1, tiled=True)
    mixed = jnp.dot(
        own_rows,
        lax.all_gather(w_out, "tp", axis=0, tiled=True),
        preferred_element_type=jnp.float32,
    )
    resid = (residual.astype(jnp.float32) + mixed).astype(jnp.bfloat16)
    resid_f = resid.astype(jnp.float32)
    normed = (
        resid_f
        * lax.rsqrt(jnp.mean(resid_f * resid_f, axis=-1, keepdims=True) + norm_eps)
        * ffn_gain
    ).astype(jnp.bfloat16)
    return moe(
        normed, resid, expert_ids.T, expert_weight.T, exp_gate, exp_up, exp_down,
        shared_gate, shared_up, shared_down,
    )


def solution(mesh):
    placed = (
        P("sp", "tp"),
        P("sp", "tp"),
        P("sp", "tp"),
        P("sp"),
        P("tp"),
        P("tp", None),
        P(("sp", "tp"), None),
        P(),
        P(("sp", "tp"), None),
        P(("sp", "tp"), None),
        P("sp", None, None),
        P("sp", None, None),
        P("sp", None, None),
        P(None, "tp"),
        P(None, "tp"),
        P("tp", None),
    )
    return jax.shard_map(
        shards, mesh=mesh, in_specs=placed, out_specs=P(("sp", "tp"), None), check_vma=False
    )
```

```python
import functools

import jax
import jax.numpy as jnp
from jax import lax
from jax.experimental import pallas as pl
from jax.experimental.pallas import tpu as pltpu
from jax.sharding import PartitionSpec as P

HD = 64
WINDOW = 128
NZ, NY, NC, NX = 8, 4, 2, 4
PLANE = NY * NC
SP = NZ * PLANE
SPAN = 512
BLOCKS = SPAN // WINDOW
HEADS = 4
OUT_ROWS = HEADS * HD
ROWS = 128
HALF = 64
CAP = 12
SLOTS = 2 * CAP
PACK = PLANE * SLOTS
D = 2048
FF = 512
EXPERTS = 64
MESH = pl.DeviceIdType.MESH
BF = jnp.bfloat16
F32 = jnp.float32

norm_eps = 1e-06


def dot(a, b):
    return jnp.dot(a, b, preferred_element_type=F32)


def silu(v):
    return v / (1.0 + jnp.exp(-v))


def chunk_of(delta):
    return 0 if delta == 0 else (2 * delta - 1 if delta <= NZ // 2 else 2 * (NZ - delta))


def layer_kernel(
    q, k, v, docs, sink, wout, residual, gain, ids, weight, eg, eu, ed, shg, shu, shd, out,
    qv, ekv, edoc, attn, atf, wo, resid,
    tok, tx, rx, ret, rst, rsx, info, inf, wg, wu, wd, sg, su, sd, sacc, hid,
    h_s, h_r, a_s, a_r, o_s, o_r, f_s, f_r,
    z_s, z_r, i_s, i_r, d_s, d_r, e_s, e_r, p_s, p_r, x_s, x_r, w_s,
):
    sp, x = lax.axis_index("sp"), lax.axis_index("tp")
    z, mine = sp // PLANE, sp % PLANE
    core = sp % NC
    twin = (sp + 1 - 2 * core, x)

    def at_sp(step):
        return ((sp + step) % SP, x)

    def at_z(dz):
        return ((z + dz) % NZ * PLANE + mine, x)

    def at_plane(j):
        return (z * PLANE + j, x)

    def at_x(dx):
        return (sp, (x + dx) % NX)

    def send(src, dst, ssem, rsem, device):
        copy = pltpu.make_async_remote_copy(
            src_ref=src, dst_ref=dst, send_sem=ssem, recv_sem=rsem, device_id=device, device_id_type=MESH
        )
        copy.start()

    def landed(ref, sem):
        pltpu.make_async_copy(ref, ref, sem).wait()

    local = [
        pltpu.make_async_copy(q, qv, w_s.at[0]),
        pltpu.make_async_copy(wout, wo.at[0], w_s.at[1]),
        pltpu.make_async_copy(residual, resid, w_s.at[2]),
        pltpu.make_async_copy(shg, sg.at[0], w_s.at[3]),
        pltpu.make_async_copy(shu, su.at[0], w_s.at[4]),
        pltpu.make_async_copy(shd, sd.at[0], w_s.at[5]),
        pltpu.make_async_copy(eg.at[0], wg, w_s.at[6]),
        pltpu.make_async_copy(eu.at[0], wu, w_s.at[7]),
        pltpu.make_async_copy(ed.at[0], wd, w_s.at[8]),
    ]
    for copy in local:
        copy.start()

    barrier = pltpu.get_barrier_semaphore()
    peers = [at_z(dz) for dz in range(1, NZ)] + [at_x(dx) for dx in range(1, NX)]
    peers += [at_plane((mine + off) % PLANE) for off in range(1, PLANE)]
    peers += [at_sp(1), at_sp(SP - 1)]
    for device in peers:
        pl.semaphore_signal(barrier, inc=1, device_id=device, device_id_type=MESH)

    ekv[pl.ds(WINDOW, SPAN), :] = jnp.concatenate([k[...], v[...]], axis=1)
    for b in range(BLOCKS):
        edoc[b + 1] = jnp.broadcast_to(docs[b : b + 1, :].astype(F32), (8, ROWS))

    pl.semaphore_wait(barrier, len(peers))
    send(ekv.at[pl.ds(WINDOW, WINDOW)], ekv.at[pl.ds(WINDOW + SPAN, WINDOW)], h_s.at[0], h_r.at[0], at_sp(SP - 1))
    send(edoc.at[1], edoc.at[BLOCKS + 1], h_s.at[1], h_r.at[1], at_sp(SP - 1))
    send(ekv.at[pl.ds(SPAN, WINDOW)], ekv.at[pl.ds(0, WINDOW)], h_s.at[2], h_r.at[2], at_sp(1))
    send(edoc.at[BLOCKS], edoc.at[0], h_s.at[3], h_r.at[3], at_sp(1))
    own_half = pl.ds(pl.multiple_of(core * (OUT_ROWS // NC), OUT_ROWS // NC), OUT_ROWS // NC)
    local[1].wait()
    for dx in (1, 3, 2):
        send(wo.at[0, own_half], wo.at[dx, own_half], o_s.at[dx], o_r.at[dx], at_x(dx))

    expert = lax.broadcasted_iota(jnp.int32, (EXPERTS, ROWS), 0)
    hits = jnp.zeros((EXPERTS, ROWS), F32)
    wide = jnp.zeros((EXPERTS, ROWS), F32)
    for k in range(ids.shape[0]):
        named = ids[k : k + 1, :] == expert
        hits = hits + named.astype(F32)
        wide = wide + jnp.where(named, weight[k : k + 1, :], 0.0)
    row = lax.broadcasted_iota(jnp.int32, (ROWS, ROWS), 0)
    col = lax.broadcasted_iota(jnp.int32, (ROWS, ROWS), 1)
    earlier = ((row < col) & (row // HALF == col // HALF)).astype(BF)
    rank = dot(hits.astype(BF), earlier)
    half = lax.broadcasted_iota(jnp.int32, (EXPERTS, ROWS), 1) // HALF
    place = jnp.where(hits > 0.0, rank + (half * CAP).astype(F32), -1.0)
    for plane in range(NZ):
        lower = plane * PLANE
        info[plane, 0:PLANE, :] = place[lower : lower + PLANE]
        info[plane, PLANE : 2 * PLANE, :] = wide[lower : lower + PLANE]
    inf[0] = info[z]

    def attention(n, carry):
        b = jnp.where(n < 3, (n + 1) % 3, 3)

        @pl.when(n == 2)
        def _():
            landed(ekv.at[pl.ds(WINDOW + SPAN, WINDOW)], h_r.at[0])
            landed(edoc.at[BLOCKS + 1], h_r.at[1])
            landed(ekv.at[pl.ds(0, WINDOW)], h_r.at[2])
            landed(edoc.at[0], h_r.at[3])

            @pl.when(sp == 0)
            def _():
                edoc[0] = jnp.full((8, ROWS), -1.0, F32)

            @pl.when(sp == SP - 1)
            def _():
                edoc[BLOCKS + 1] = jnp.full((8, ROWS), -1.0, F32)

        rows = pl.ds(pl.multiple_of(b * WINDOW, WINDOW), WINDOW)
        band = ekv[pl.ds(pl.multiple_of(b * WINDOW, WINDOW), 3 * WINDOW), :]
        own_doc = jnp.broadcast_to(edoc[b + 1][0:1, :], (WINDOW, WINDOW)).T
        at_row = lax.broadcasted_iota(jnp.int32, (WINDOW, WINDOW), 0)
        at_col = lax.broadcasted_iota(jnp.int32, (WINDOW, WINDOW), 1)
        near = (at_col >= at_row, at_row >= 0, at_col <= at_row)
        allowed = jnp.concatenate(
            [
                ((own_doc == edoc[b + t][0:1, :]) & near[t]).astype(F32)
                for t in range(3)
            ],
            axis=1,
        )
        heads = []
        for h in range(HEADS):
            query = qv[rows, h * HD : (h + 1) * HD]
            scores = lax.dot_general(
                query, band[:, :HD], (((1,), (1,)), ((), ())), preferred_element_type=F32
            ) * HD ** (-0.5)
            scores = jnp.where(allowed > 0.0, scores, -jnp.inf)
            row_max = jnp.maximum(jnp.max(scores, axis=1, keepdims=True), sink[h])
            grown = jnp.exp(scores - row_max)
            total = jnp.sum(grown, axis=1, keepdims=True) + jnp.exp(sink[h] - row_max)
            heads.append(dot((grown / total).astype(BF), band[:, HD:]).astype(BF))
        attn[b] = jnp.concatenate(heads, axis=1)
        slot = (b + NX - x) % NX

        @pl.when(b != x)
        def _():
            send(attn.at[b], atf.at[slot], a_s.at[slot], a_r.at[slot], (sp, b))

        @pl.when(b == x)
        def _():
            pltpu.make_async_copy(attn.at[b], atf.at[0], a_r.at[0]).start()

        return carry

    local[0].wait()
    lax.fori_loop(0, BLOCKS, attention, 0)

    for dx in (1, 3, 2):
        landed(wo.at[dx, own_half], o_r.at[dx])
        send(wo.at[dx, own_half], wo.at[dx, own_half], f_s.at[dx], f_r.at[dx], twin)
    local[2].wait()
    other_half = pl.ds(
        pl.multiple_of((1 - core) * (OUT_ROWS // NC), OUT_ROWS // NC), OUT_ROWS // NC
    )
    landed(atf.at[0], a_r.at[0])
    for dx in (1, 3, 2):
        landed(atf.at[dx], a_r.at[dx])
        landed(wo.at[dx, other_half], f_r.at[dx])

    def project(n, squares):
        cols = pl.ds(pl.multiple_of(n * 256, 256), 256)
        mixed = dot(atf[0], wo[0, :, cols])
        for dx in range(1, NX):
            mixed = mixed + dot(atf[dx], wo[dx, :, cols])
        rounded = (resid[:, cols].astype(F32) + mixed).astype(BF)
        resid[:, cols] = rounded
        squared = rounded.astype(F32)
        squared = squared * squared
        return squares + squared[:, :128] + squared[:, 128:]

    squares = lax.fori_loop(0, D // 256, project, jnp.zeros((ROWS, 128), F32))
    scale = lax.rsqrt(jnp.sum(squares, axis=1, keepdims=True) * (1.0 / D) + norm_eps)
    for n in range(D // 512):
        cols = pl.ds(n * 512, 512)
        tok[0, :, cols] = (resid[:, cols].astype(F32) * scale * gain[:, cols]).astype(BF)

    for delta in range(1, NZ):
        i = chunk_of(delta)
        send(info.at[(z + delta) % NZ], inf.at[i], i_s.at[i], i_r.at[i], at_z(delta))
    send(tok.at[0], tok.at[1], z_s.at[1], z_r.at[1], at_z(1))
    send(tok.at[0], tok.at[2], z_s.at[2], z_r.at[2], at_z(NZ - 1))

    def placed(i):
        slot = lax.broadcasted_iota(jnp.int32, (PLANE, SLOTS, ROWS), 1).astype(F32)
        return (inf[i, 0:PLANE, :][:, None, :] == slot).astype(F32)

    def dispatch(i):
        @pl.when(i > 0)
        def _():
            landed(tok.at[i], z_r.at[i])
            landed(inf.at[i], i_r.at[i])

        @pl.when((i > 0) & (i + 2 < NZ))
        def _():
            way = 1 + (NZ - 2) * ((i + 1) % 2)
            send(tok.at[i], tok.at[i + 2], z_s.at[i + 2], z_r.at[i + 2], at_z(way))

        pick = placed(i).reshape(PACK, ROWS).astype(BF)
        for n in range(D // 512):
            cols = pl.ds(n * 512, 512)
            tx[i, :, :, cols] = dot(pick, tok[i, :, cols]).astype(BF).reshape(PLANE, SLOTS, 512)
        for off in range(1, PLANE):
            j = (mine + off) % PLANE
            send(tx.at[i, j], rx.at[i, mine], d_s.at[i], d_r.at[i], at_plane(j))
        pltpu.make_async_copy(tx.at[i, mine], rx.at[i, mine], d_r.at[i]).start()

    def run_expert(i):
        landed(rx.at[i], d_r.at[i])

        def hidden_tile(n, carry):
            cols = pl.ds(pl.multiple_of(n * 256, 256), 256)
            rows = rx[i].reshape(PACK, D)
            hid[:, cols] = (silu(dot(rows, wg[:, cols])) * dot(rows, wu[:, cols])).astype(BF)
            return carry

        lax.fori_loop(0, FF // 256, hidden_tile, 0)

        def out_tile(n, carry):
            cols = pl.ds(pl.multiple_of(n * 512, 512), 512)
            rx[i, :, :, cols] = dot(hid[...], wd[:, cols]).astype(BF).reshape(PLANE, SLOTS, 512)
            return carry

        lax.fori_loop(0, D // 512, out_tile, 0)

    def give_back(i):
        for off in range(1, PLANE):
            j = (mine + off) % PLANE
            send(rx.at[i, j], ret.at[i, mine], e_s.at[i], e_r.at[i], at_plane(j))
        pltpu.make_async_copy(rx.at[i, mine], ret.at[i, mine], e_r.at[i]).start()

    LAG = 2

    def forward(i, carry):
        @pl.when(i < NZ)
        def _():
            dispatch(i)

        @pl.when(i == 0)
        def _():
            for dx in range(1, NX):
                send(sg.at[0], sg.at[dx], x_s.at[0, dx], x_r.at[0, dx], at_x(dx))
                send(su.at[0], su.at[dx], x_s.at[1, dx], x_r.at[1, dx], at_x(dx))
                send(sd.at[0], sd.at[dx], x_s.at[2, dx], x_r.at[2, dx], at_x(dx))

        @pl.when(i >= LAG)
        def _():
            run_expert(i - LAG)

        @pl.when(i >= NZ - 2 + LAG)
        def _():
            give_back(i - LAG)

        return carry

    for copy in local[3:]:
        copy.wait()
    lax.fori_loop(0, NZ + LAG, forward, 0)

    def backward(n, carry):
        give_back(NZ - 3 - n)
        return carry

    lax.fori_loop(0, NZ - 2, backward, 0)

    for dx in range(1, NX):
        landed(sg.at[dx], x_r.at[0, dx])
        landed(su.at[dx], x_r.at[1, dx])
        landed(sd.at[dx], x_r.at[2, dx])
    sacc[...] = jnp.zeros_like(sacc)

    def shared_block(dx, carry):
        rows = tok[0]
        units = (silu(dot(rows, sg[dx])) * dot(rows, su[dx])).astype(BF)
        for n in range(D // 512):
            cols = pl.ds(n * 512, 512)
            sacc[:, cols] = sacc[:, cols] + dot(units, sd[dx, :, cols])
        return carry

    lax.fori_loop(0, NX, shared_block, 0)

    def combined(i):
        landed(ret.at[i], e_r.at[i])
        scaled = placed(i) * inf[i, PLANE : 2 * PLANE, :][:, None, :]
        scaled = jnp.concatenate([scaled.reshape(PACK, ROWS), jnp.zeros((256 - PACK, ROWS), F32)], axis=0)
        scaled = scaled.T[:, :PACK]
        high = scaled.astype(BF)
        low = (scaled - high.astype(F32)).astype(BF)

        def part(cols):
            rows = ret[i, :, :, cols].reshape(PACK, 512)
            return dot(high, rows) + dot(low, rows)

        return part

    def pass_on(i):
        way = NZ - 1 - (NZ - 2) * ((i + 1) % 2)
        send(rst.at[i], rsx.at[i], p_s.at[i], p_r.at[i], at_z(way))

    def farthest(n, carry):
        i = NZ - 1 - n
        part = combined(i)
        for n in range(D // 512):
            cols = pl.ds(n * 512, 512)
            rst[i, :, cols] = part(cols).astype(BF)
        pass_on(i)
        return carry

    lax.fori_loop(0, 2, farthest, 0)

    def nearer(n, carry):
        i = NZ - 3 - n
        part = combined(i)
        landed(rsx.at[i + 2], p_r.at[i + 2])
        for n in range(D // 512):
            cols = pl.ds(n * 512, 512)
            rst[i, :, cols] = (part(cols) + rsx[i + 2, :, cols].astype(F32)).astype(BF)
        pass_on(i)
        return carry

    lax.fori_loop(0, NZ - 3, nearer, 0)

    part = combined(0)
    landed(rsx.at[2], p_r.at[2])
    landed(rsx.at[1], p_r.at[1])
    for n in range(D // 512):
        cols = pl.ds(n * 512, 512)
        routed = part(cols) + rsx[2, :, cols].astype(F32) + rsx[1, :, cols].astype(F32)
        out[:, cols] = (resid[:, cols].astype(F32) + sacc[:, cols] + routed).astype(BF)

    for i in range(NZ):
        landed(tx.at[i, pl.ds(0, PLANE - 1)], d_s.at[i])
        landed(rx.at[i, pl.ds(0, PLANE - 1)], e_s.at[i])
        if i > 0:
            landed(tok.at[i], z_s.at[i])
            landed(info.at[i], i_s.at[i])
            landed(rst.at[i], p_s.at[i])
    landed(ekv.at[pl.ds(0, WINDOW)], h_s.at[0])
    landed(edoc.at[0], h_s.at[1])
    landed(ekv.at[pl.ds(0, WINDOW)], h_s.at[2])
    landed(edoc.at[0], h_s.at[3])
    for dx in range(1, NX):
        landed(atf.at[0], a_s.at[dx])
        landed(wo.at[0, pl.ds(0, OUT_ROWS // NC)], o_s.at[dx])
        landed(wo.at[0, pl.ds(0, OUT_ROWS // NC)], f_s.at[dx])
        landed(sg.at[0], x_s.at[0, dx])
        landed(su.at[0], x_s.at[1, dx])
        landed(sd.at[0], x_s.at[2, dx])


def shards(
    queries,
    keys,
    values,
    doc_ids,
    sink_logit,
    w_out,
    residual,
    ffn_gain,
    expert_ids,
    expert_weight,
    exp_gate,
    exp_up,
    exp_down,
    shared_gate,
    shared_up,
    shared_down,
):
    vmem = pl.BlockSpec(memory_space=pltpu.VMEM)
    smem = pl.BlockSpec(memory_space=pltpu.SMEM)
    hbm = pl.BlockSpec(memory_space=pl.ANY)
    dma = pltpu.SemaphoreType.DMA
    unit = FF // NX
    return pl.pallas_call(
        layer_kernel,
        out_shape=jax.ShapeDtypeStruct((ROWS, D), BF),
        in_specs=[hbm, vmem, vmem, vmem, smem, hbm, hbm, vmem, vmem, vmem] + [hbm] * 6,
        out_specs=vmem,
        scratch_shapes=[
            pltpu.VMEM((SPAN, HEADS * HD), BF),
            pltpu.VMEM((SPAN + 2 * WINDOW, 2 * HD), BF),
            pltpu.VMEM((BLOCKS + 2, 8, ROWS), F32),
            pltpu.VMEM((BLOCKS, ROWS, HEADS * HD), BF),
            pltpu.VMEM((NX, ROWS, HEADS * HD), BF),
            pltpu.VMEM((NX, OUT_ROWS, D), BF),
            pltpu.VMEM((ROWS, D), BF),
            pltpu.VMEM((NZ, ROWS, D), BF),
            pltpu.VMEM((NZ, PLANE, SLOTS, D), BF),
            pltpu.VMEM((NZ, PLANE, SLOTS, D), BF),
            pltpu.VMEM((NZ, PLANE, SLOTS, D), BF),
            pltpu.VMEM((NZ, ROWS, D), BF),
            pltpu.VMEM((NZ, ROWS, D), BF),
            pltpu.VMEM((NZ, 2 * PLANE, ROWS), F32),
            pltpu.VMEM((NZ, 2 * PLANE, ROWS), F32),
            pltpu.VMEM((D, FF), BF),
            pltpu.VMEM((D, FF), BF),
            pltpu.VMEM((FF, D), BF),
            pltpu.VMEM((NX, D, unit), BF),
            pltpu.VMEM((NX, D, unit), BF),
            pltpu.VMEM((NX, unit, D), BF),
            pltpu.VMEM((ROWS, D), F32),
            pltpu.VMEM((PACK, FF), BF),
        ]
        + [dma((4,))] * 8
        + [dma((NZ,))] * 10
        + [dma((3, NX)), dma((3, NX)), dma((9,))],
        compiler_params=pltpu.CompilerParams(
            collective_id=1, has_side_effects=True, vmem_limit_bytes=62 * 2**20
        ),
        name="layer",
    )(
        queries, keys, values, doc_ids.reshape(BLOCKS, ROWS), sink_logit, w_out, residual,
        ffn_gain.reshape(1, D), expert_ids.T, expert_weight.T,
        exp_gate, exp_up, exp_down, shared_gate, shared_up, shared_down,
    )


def solution(mesh):
    placed = (
        P("sp", "tp"),
        P("sp", "tp"),
        P("sp", "tp"),
        P("sp"),
        P("tp"),
        P("tp", None),
        P(("sp", "tp"), None),
        P(),
        P(("sp", "tp"), None),
        P(("sp", "tp"), None),
        P("sp", None, None),
        P("sp", None, None),
        P("sp", None, None),
        P(None, "tp"),
        P(None, "tp"),
        P("tp", None),
    )
    return jax.shard_map(
        shards, mesh=mesh, in_specs=placed, out_specs=P(("sp", "tp"), None), check_vma=False
    )
```

```python
import functools

import jax
import jax.numpy as jnp
from jax import lax
from jax.experimental import pallas as pl
from jax.experimental.pallas import tpu as pltpu
from jax.sharding import PartitionSpec as P

HD = 64
WINDOW = 128
NZ, NY, NC, NX = 8, 4, 2, 4
PLANE = NY * NC
SP = NZ * PLANE
SPAN = 512
BLOCKS = SPAN // WINDOW
HEADS = 4
OUT_ROWS = HEADS * HD
OUT_HALF = OUT_ROWS // NC
DIRECT = 64
SHARE = (OUT_HALF - DIRECT) // NY
PART = 1024
ROWS = 128
HALF = 64
CAP = 12
SLOTS = 2 * CAP
PACK = PLANE * SLOTS
D = 2048
FF = 512
EXPERTS = 64
MESH = pl.DeviceIdType.MESH
BF = jnp.bfloat16
F32 = jnp.float32

norm_eps = 1e-06


def dot(a, b):
    return jnp.dot(a, b, preferred_element_type=F32)


def silu(v):
    return v / (1.0 + jnp.exp(-v))


def chunk_of(delta):
    return 0 if delta == 0 else (2 * delta - 1 if delta <= NZ // 2 else 2 * (NZ - delta))


def layer_kernel(
    q, k, v, docs, sink, wout, residual, gain, ids, weight, eg, eu, ed, shg, shu, shd, out,
    qv, ekv, edoc, attn, atf, wo, resid,
    tok, tx, rx, ret, rst, rsx, info, inf, wg, wu, wd, sg, su, sd, sacc, hid,
    h_s, h_r, a_s, a_r, o_s, o_r, f_s, f_r, g_s, g_r,
    z_s, z_r, i_s, i_r, d_s, d_r, e_s, e_r, p_s, p_r, x_s, x_r, w_s,
):
    sp, x = lax.axis_index("sp"), lax.axis_index("tp")
    z, mine = sp // PLANE, sp % PLANE
    core = sp % NC
    twin = (sp + 1 - 2 * core, x)

    def at_sp(step):
        return ((sp + step) % SP, x)

    def at_z(dz):
        return ((z + dz) % NZ * PLANE + mine, x)

    def at_plane(j):
        return (z * PLANE + j, x)

    def at_x(dx):
        return (sp, (x + dx) % NX)

    def send(src, dst, ssem, rsem, device):
        copy = pltpu.make_async_remote_copy(
            src_ref=src, dst_ref=dst, send_sem=ssem, recv_sem=rsem, device_id=device, device_id_type=MESH
        )
        copy.start()

    def landed(ref, sem):
        pltpu.make_async_copy(ref, ref, sem).wait()

    local = [
        pltpu.make_async_copy(q, qv, w_s.at[0]),
        pltpu.make_async_copy(residual, resid, w_s.at[1]),
        pltpu.make_async_copy(wout, wo.at[0], w_s.at[2]),
        pltpu.make_async_copy(shg, sg.at[0], w_s.at[3]),
        pltpu.make_async_copy(shu, su.at[0], w_s.at[4]),
        pltpu.make_async_copy(shd, sd.at[0], w_s.at[5]),
        pltpu.make_async_copy(eg.at[0], wg, w_s.at[6]),
        pltpu.make_async_copy(eu.at[0], wu, w_s.at[7]),
        pltpu.make_async_copy(ed.at[0], wd, w_s.at[8]),
    ]
    for copy in local[:2]:
        copy.start()

    barrier = pltpu.get_barrier_semaphore()
    peers = [at_z(dz) for dz in range(1, NZ)] + [at_x(dx) for dx in range(1, NX)]
    peers += [at_plane((mine + off) % PLANE) for off in range(1, PLANE)]
    peers += [at_sp(1), at_sp(SP - 1)]
    for device in peers:
        pl.semaphore_signal(barrier, inc=1, device_id=device, device_id_type=MESH)

    ekv[0:HD, pl.ds(WINDOW, SPAN)] = k[...]
    ekv[HD : 2 * HD, pl.ds(WINDOW, SPAN)] = v[...]
    for b in range(BLOCKS):
        edoc[b + 1] = jnp.broadcast_to(docs[b : b + 1, :].astype(F32), (8, ROWS))

    pl.semaphore_wait(barrier, len(peers))
    send(ekv.at[:, pl.ds(WINDOW, WINDOW)], ekv.at[:, pl.ds(WINDOW + SPAN, WINDOW)], h_s.at[0], h_r.at[0], at_sp(SP - 1))
    send(edoc.at[1], edoc.at[BLOCKS + 1], h_s.at[1], h_r.at[1], at_sp(SP - 1))
    send(ekv.at[:, pl.ds(SPAN, WINDOW)], ekv.at[:, pl.ds(0, WINDOW)], h_s.at[2], h_r.at[2], at_sp(1))
    send(edoc.at[BLOCKS], edoc.at[0], h_s.at[3], h_r.at[3], at_sp(1))
    lower = core * OUT_HALF
    direct = pl.ds(pl.multiple_of(lower, OUT_HALF), DIRECT)
    spread = pl.ds(pl.multiple_of(lower + DIRECT, SHARE), OUT_HALF - DIRECT)
    share = pl.ds(pl.multiple_of(lower + DIRECT + mine // NC * SHARE, SHARE), SHARE)
    others = pl.ds(1, NX - 1)
    for dx in (1, 3, 2):
        send(wout.at[share], wo.at[dx, share], g_s.at[0, dx], g_r.at[0, dx], at_x(dx))
    for dx in (1, 3, 2):
        send(wout.at[direct], wo.at[dx, direct], o_s.at[dx], o_r.at[dx], at_x(dx))

    expert = lax.broadcasted_iota(jnp.int32, (EXPERTS, ROWS), 0)
    hits = jnp.zeros((EXPERTS, ROWS), F32)
    wide = jnp.zeros((EXPERTS, ROWS), F32)
    for k in range(ids.shape[0]):
        named = ids[k : k + 1, :] == expert
        hits = hits + named.astype(F32)
        wide = wide + jnp.where(named, weight[k : k + 1, :], 0.0)
    row = lax.broadcasted_iota(jnp.int32, (ROWS, ROWS), 0)
    col = lax.broadcasted_iota(jnp.int32, (ROWS, ROWS), 1)
    earlier = ((row < col) & (row // HALF == col // HALF)).astype(BF)
    rank = dot(hits.astype(BF), earlier)
    half = lax.broadcasted_iota(jnp.int32, (EXPERTS, ROWS), 1) // HALF
    place = jnp.where(hits > 0.0, rank + (half * CAP).astype(F32), -1.0)
    for plane in range(NZ):
        lower = plane * PLANE
        info[plane, 0:PLANE, :] = place[lower : lower + PLANE]
        info[plane, PLANE : 2 * PLANE, :] = wide[lower : lower + PLANE]
    inf[0] = info[z]

    def attention(n, carry):
        b = jnp.where(n < 3, (n + 1) % 3, 3)

        @pl.when(n == 2)
        def _():
            landed(ekv.at[:, pl.ds(WINDOW + SPAN, WINDOW)], h_r.at[0])
            landed(edoc.at[BLOCKS + 1], h_r.at[1])
            landed(ekv.at[:, pl.ds(0, WINDOW)], h_r.at[2])
            landed(edoc.at[0], h_r.at[3])

            @pl.when(sp == 0)
            def _():
                edoc[0] = jnp.full((8, ROWS), -1.0, F32)

            @pl.when(sp == SP - 1)
            def _():
                edoc[BLOCKS + 1] = jnp.full((8, ROWS), -1.0, F32)

        rows = pl.ds(pl.multiple_of(b * WINDOW, WINDOW), WINDOW)
        band = ekv[:, pl.ds(pl.multiple_of(b * WINDOW, WINDOW), 3 * WINDOW)]
        own_doc = jnp.broadcast_to(edoc[b + 1][0:1, :], (WINDOW, WINDOW)).T
        at_row = lax.broadcasted_iota(jnp.int32, (WINDOW, WINDOW), 0)
        at_col = lax.broadcasted_iota(jnp.int32, (WINDOW, WINDOW), 1)
        near = (at_col >= at_row, at_row >= 0, at_col <= at_row)
        allowed = jnp.concatenate(
            [
                ((own_doc == edoc[b + t][0:1, :]) & near[t]).astype(F32)
                for t in range(3)
            ],
            axis=1,
        )
        heads = []
        for h in range(HEADS):
            query = qv[rows, h * HD : (h + 1) * HD]
            scores = dot(query, band[:HD]) * HD ** (-0.5)
            scores = jnp.where(allowed > 0.0, scores, -jnp.inf)
            row_max = jnp.maximum(jnp.max(scores, axis=1, keepdims=True), sink[h])
            grown = jnp.exp(scores - row_max)
            total = jnp.sum(grown, axis=1, keepdims=True) + jnp.exp(sink[h] - row_max)
            probs = (grown / total).astype(BF)
            mixed = lax.dot_general(probs, band[HD:], (((1,), (1,)), ((), ())), preferred_element_type=F32)
            heads.append(mixed.astype(BF))
        attn[b] = jnp.concatenate(heads, axis=1)
        slot = (b + NX - x) % NX

        @pl.when(b != x)
        def _():
            send(attn.at[b], atf.at[slot], a_s.at[slot], a_r.at[slot], (sp, b))

        @pl.when(b == x)
        def _():
            pltpu.make_async_copy(attn.at[b], atf.at[0], a_r.at[0]).start()

        return carry

    local[0].wait()
    lax.fori_loop(0, BLOCKS, attention, 0)

    for copy in local[2:]:
        copy.start()
    for dx in (1, 3, 2):
        landed(wo.at[dx, share], g_r.at[0, dx])
    for dy in range(1, NY):
        send(wo.at[others, share], wo.at[others, share], g_s.at[1, dy], g_r.at[1, dy], at_plane((mine + NC * dy) % PLANE))
    for dx in (1, 3, 2):
        landed(wo.at[dx, direct], o_r.at[dx])
    send(wo.at[others, direct], wo.at[others, direct], f_s.at[0], f_r.at[0], twin)
    for dy in range(1, NY):
        landed(wo.at[others, share], g_r.at[1, dy])
    send(wo.at[others, spread], wo.at[others, spread], f_s.at[1], f_r.at[1], twin)
    local[1].wait()
    local[2].wait()
    for dx in range(NX):
        landed(atf.at[dx], a_r.at[dx])
    landed(wo.at[others, direct], f_r.at[0])
    landed(wo.at[others, spread], f_r.at[1])

    def project(n, squares):
        cols = pl.ds(pl.multiple_of(n * 256, 256), 256)
        mixed = dot(atf[0], wo[0, :, cols])
        for dx in range(1, NX):
            mixed = mixed + dot(atf[dx], wo[dx, :, cols])
        rounded = (resid[:, cols].astype(F32) + mixed).astype(BF)
        resid[:, cols] = rounded
        squared = rounded.astype(F32)
        squared = squared * squared
        return squares + squared[:, :128] + squared[:, 128:]

    squares = lax.fori_loop(0, D // 256, project, jnp.zeros((ROWS, 128), F32))
    scale = lax.rsqrt(jnp.sum(squares, axis=1, keepdims=True) * (1.0 / D) + norm_eps)
    for h in range(2):
        cols = pl.ds(h * PART, PART)
        tok[0, h] = (resid[:, cols].astype(F32) * scale * gain[:, cols]).astype(BF)

    for delta in range(1, NZ):
        i = chunk_of(delta)
        send(info.at[(z + delta) % NZ], inf.at[i], i_s.at[i], i_r.at[i], at_z(delta))
    for h in range(2):
        send(tok.at[0, h], tok.at[1, h], z_s.at[1, h], z_r.at[1, h], at_z(1))
        send(tok.at[0, h], tok.at[2, h], z_s.at[2, h], z_r.at[2, h], at_z(NZ - 1))

    def placed(i):
        slot = lax.broadcasted_iota(jnp.int32, (PLANE, SLOTS, ROWS), 1).astype(F32)
        return (inf[i, 0:PLANE, :][:, None, :] == slot).astype(F32)

    def dispatch(i, h):
        @pl.when(i > 0)
        def _():
            landed(tok.at[i, h], z_r.at[i, h])

            @pl.when(h == 0)
            def _():
                landed(inf.at[i], i_r.at[i])

        @pl.when((i > 0) & (i + 2 < NZ))
        def _():
            way = 1 + (NZ - 2) * ((i + 1) % 2)
            send(tok.at[i, h], tok.at[i + 2, h], z_s.at[i + 2, h], z_r.at[i + 2, h], at_z(way))

        pick = placed(i).reshape(PACK, ROWS).astype(BF)
        for n in range(PART // 512):
            cols = pl.ds(n * 512, 512)
            tx[i, h, :, :, cols] = dot(pick, tok[i, h, :, cols]).astype(BF).reshape(PLANE, SLOTS, 512)
        for off in range(1, PLANE):
            j = (mine + off) % PLANE
            send(tx.at[i, h, j], rx.at[i, h, mine], d_s.at[i], d_r.at[i], at_plane(j))
        pltpu.make_async_copy(tx.at[i, h, mine], rx.at[i, h, mine], d_r.at[i]).start()

    def run_expert(i):
        landed(rx.at[i], d_r.at[i])

        def hidden_tile(n, carry):
            cols = pl.ds(pl.multiple_of(n * 256, 256), 256)
            left, right = rx[i, 0].reshape(PACK, PART), rx[i, 1].reshape(PACK, PART)
            gate = dot(left, wg[0:PART, cols]) + dot(right, wg[PART:D, cols])
            up = dot(left, wu[0:PART, cols]) + dot(right, wu[PART:D, cols])
            hid[:, cols] = (silu(gate) * up).astype(BF)
            return carry

        lax.fori_loop(0, FF // 256, hidden_tile, 0)

        def out_tile(n, carry):
            cols = pl.ds(pl.multiple_of(n * 512, 512), 512)
            made = dot(hid[...], wd[:, cols]).astype(BF).reshape(PLANE, SLOTS, 512)
            rx[i, n // 2, :, :, pl.ds(pl.multiple_of(n % 2 * 512, 512), 512)] = made
            return carry

        lax.fori_loop(0, D // 512, out_tile, 0)

    def give_back(i):
        for h in range(2):
            for off in range(1, PLANE):
                j = (mine + off) % PLANE
                send(rx.at[i, h, j], ret.at[i, h, mine], e_s.at[i, h], e_r.at[i, h], at_plane(j))
            pltpu.make_async_copy(rx.at[i, h, mine], ret.at[i, h, mine], e_r.at[i, h]).start()

    def pieces(n, carry):
        m = jnp.maximum(n - 2, 0)
        i = jnp.where(n < 2, 0, 1 + m // 4 * 2 + m % 2)
        h = jnp.where(n < 2, n, m % 4 // 2)

        @pl.when(i < NZ)
        def _():
            dispatch(i, h)

        @pl.when(n == 1)
        def _():
            for copy in local[3:6]:
                copy.wait()
            for dx in range(1, NX):
                send(sg.at[0], sg.at[dx], x_s.at[0, dx], x_r.at[0, dx], at_x(dx))
                send(su.at[0], su.at[dx], x_s.at[1, dx], x_r.at[1, dx], at_x(dx))
                send(sd.at[0], sd.at[dx], x_s.at[2, dx], x_r.at[2, dx], at_x(dx))
            for copy in local[6:]:
                copy.wait()

        @pl.when((n == 9) | (n == 13))
        def _():
            def early(j, carry):
                run_expert((n - 9) // 2 + j)
                return carry

            lax.fori_loop(0, 2, early, 0)

        return carry

    lax.fori_loop(0, 2 + 2 * NZ, pieces, 0)

    def late(j, carry):
        run_expert(j)

        @pl.when(j >= NZ - 2)
        def _():
            give_back(j)

        return carry

    lax.fori_loop(4, NZ, late, 0)

    def backward(n, carry):
        give_back(NZ - 3 - n)
        return carry

    lax.fori_loop(0, NZ - 2, backward, 0)

    for dx in range(1, NX):
        landed(sg.at[dx], x_r.at[0, dx])
        landed(su.at[dx], x_r.at[1, dx])
        landed(sd.at[dx], x_r.at[2, dx])
    sacc[...] = jnp.zeros_like(sacc)

    def shared_block(dx, carry):
        left, right = tok[0, 0], tok[0, 1]
        gate = dot(left, sg[dx, 0:PART]) + dot(right, sg[dx, PART:D])
        up = dot(left, su[dx, 0:PART]) + dot(right, su[dx, PART:D])
        units = (silu(gate) * up).astype(BF)
        for n in range(D // 512):
            cols = pl.ds(n * 512, 512)
            sacc[:, cols] = sacc[:, cols] + dot(units, sd[dx, :, cols])
        return carry

    lax.fori_loop(0, NX, shared_block, 0)

    def combined(i):
        scaled = placed(i) * inf[i, PLANE : 2 * PLANE, :][:, None, :]
        scaled = jnp.concatenate([scaled.reshape(PACK, ROWS), jnp.zeros((256 - PACK, ROWS), F32)], axis=0)
        scaled = scaled.T[:, :PACK]
        high = scaled.astype(BF)
        low = (scaled - high.astype(F32)).astype(BF)

        def part(h, cols):
            rows = ret[i, h, :, :, cols].reshape(PACK, 512)
            return dot(high, rows) + dot(low, rows)

        return part

    def pass_on(i, h):
        way = NZ - 1 - (NZ - 2) * ((i + 1) % 2)
        send(rst.at[i, h], rsx.at[i, h], p_s.at[i, h], p_r.at[i, h], at_z(way))

    def farthest(n, carry):
        i = NZ - 2 + n
        part = combined(i)
        for h in range(2):
            landed(ret.at[i, h], e_r.at[i, h])
            for n in range(PART // 512):
                cols = pl.ds(n * 512, 512)
                rst[i, h, :, cols] = part(h, cols).astype(BF)
            pass_on(i, h)
        return carry

    lax.fori_loop(0, 2, farthest, 0)

    def nearer(n, carry):
        i = NZ - 3 - n
        part = combined(i)
        for h in range(2):
            landed(ret.at[i, h], e_r.at[i, h])
            landed(rsx.at[i + 2, h], p_r.at[i + 2, h])
            for n in range(PART // 512):
                cols = pl.ds(n * 512, 512)
                rst[i, h, :, cols] = (part(h, cols) + rsx[i + 2, h, :, cols].astype(F32)).astype(BF)
            pass_on(i, h)
        return carry

    lax.fori_loop(0, NZ - 3, nearer, 0)

    part = combined(0)
    for h in range(2):
        landed(ret.at[0, h], e_r.at[0, h])
        landed(rsx.at[2, h], p_r.at[2, h])
        landed(rsx.at[1, h], p_r.at[1, h])
        for n in range(PART // 512):
            cols, wide = pl.ds(n * 512, 512), pl.ds(h * PART + n * 512, 512)
            routed = part(h, cols) + rsx[2, h, :, cols].astype(F32) + rsx[1, h, :, cols].astype(F32)
            out[:, wide] = (resid[:, wide].astype(F32) + sacc[:, wide] + routed).astype(BF)

    for i in range(NZ):
        landed(tx.at[i, :, pl.ds(0, PLANE - 1)], d_s.at[i])
        if i > 0:
            landed(info.at[i], i_s.at[i])
        for h in range(2):
            landed(rx.at[i, h, pl.ds(0, PLANE - 1)], e_s.at[i, h])
            if i > 0:
                landed(tok.at[i, h], z_s.at[i, h])
                landed(rst.at[i, h], p_s.at[i, h])
    landed(ekv.at[:, pl.ds(0, WINDOW)], h_s.at[0])
    landed(edoc.at[0], h_s.at[1])
    landed(ekv.at[:, pl.ds(0, WINDOW)], h_s.at[2])
    landed(edoc.at[0], h_s.at[3])
    landed(wo.at[others, direct], f_s.at[0])
    landed(wo.at[others, spread], f_s.at[1])
    for dx in range(1, NX):
        landed(atf.at[0], a_s.at[dx])
        landed(wo.at[0, direct], o_s.at[dx])
        landed(wo.at[0, share], g_s.at[0, dx])
        landed(wo.at[others, share], g_s.at[1, dx])
        landed(sg.at[0], x_s.at[0, dx])
        landed(su.at[0], x_s.at[1, dx])
        landed(sd.at[0], x_s.at[2, dx])


def shards(
    queries,
    keys,
    values,
    doc_ids,
    sink_logit,
    w_out,
    residual,
    ffn_gain,
    expert_ids,
    expert_weight,
    exp_gate,
    exp_up,
    exp_down,
    shared_gate,
    shared_up,
    shared_down,
):
    vmem = pl.BlockSpec(memory_space=pltpu.VMEM)
    smem = pl.BlockSpec(memory_space=pltpu.SMEM)
    hbm = pl.BlockSpec(memory_space=pl.ANY)
    dma = pltpu.SemaphoreType.DMA
    unit = FF // NX
    return pl.pallas_call(
        layer_kernel,
        out_shape=jax.ShapeDtypeStruct((ROWS, D), BF),
        in_specs=[hbm, vmem, vmem, vmem, smem, hbm, hbm, vmem, vmem, vmem] + [hbm] * 6,
        out_specs=vmem,
        scratch_shapes=[
            pltpu.VMEM((SPAN, HEADS * HD), BF),
            pltpu.VMEM((2 * HD, SPAN + 2 * WINDOW), BF),
            pltpu.VMEM((BLOCKS + 2, 8, ROWS), F32),
            pltpu.VMEM((BLOCKS, ROWS, HEADS * HD), BF),
            pltpu.VMEM((NX, ROWS, HEADS * HD), BF),
            pltpu.VMEM((NX, OUT_ROWS, D), BF),
            pltpu.VMEM((ROWS, D), BF),
            pltpu.VMEM((NZ, 2, ROWS, PART), BF),
            pltpu.VMEM((NZ, 2, PLANE, SLOTS, PART), BF),
            pltpu.VMEM((NZ, 2, PLANE, SLOTS, PART), BF),
            pltpu.VMEM((NZ, 2, PLANE, SLOTS, PART), BF),
            pltpu.VMEM((NZ, 2, ROWS, PART), BF),
            pltpu.VMEM((NZ, 2, ROWS, PART), BF),
            pltpu.VMEM((NZ, 2 * PLANE, ROWS), F32),
            pltpu.VMEM((NZ, 2 * PLANE, ROWS), F32),
            pltpu.VMEM((D, FF), BF),
            pltpu.VMEM((D, FF), BF),
            pltpu.VMEM((FF, D), BF),
            pltpu.VMEM((NX, D, unit), BF),
            pltpu.VMEM((NX, D, unit), BF),
            pltpu.VMEM((NX, unit, D), BF),
            pltpu.VMEM((ROWS, D), F32),
            pltpu.VMEM((PACK, FF), BF),
        ]
        + [dma((4,))] * 8
        + [dma((2, NX))] * 2
        + [dma((NZ, 2))] * 2
        + [dma((NZ,))] * 4
        + [dma((NZ, 2))] * 4
        + [dma((3, NX)), dma((3, NX)), dma((9,))],
        compiler_params=pltpu.CompilerParams(
            collective_id=1, has_side_effects=True, vmem_limit_bytes=62 * 2**20
        ),
        name="layer",
    )(
        queries, keys.T, values.T, doc_ids.reshape(BLOCKS, ROWS), sink_logit, w_out, residual,
        ffn_gain.reshape(1, D), expert_ids.T, expert_weight.T,
        exp_gate, exp_up, exp_down, shared_gate, shared_up, shared_down,
    )


def solution(mesh):
    placed = (
        P("sp", "tp"),
        P("sp", "tp"),
        P("sp", "tp"),
        P("sp"),
        P("tp"),
        P("tp", None),
        P(("sp", "tp"), None),
        P(),
        P(("sp", "tp"), None),
        P(("sp", "tp"), None),
        P("sp", None, None),
        P("sp", None, None),
        P("sp", None, None),
        P(None, "tp"),
        P(None, "tp"),
        P("tp", None),
    )
    return jax.shard_map(
        shards, mesh=mesh, in_specs=placed, out_specs=P(("sp", "tp"), None), check_vma=False
    )
```

```python
import functools

import jax
import jax.numpy as jnp
from jax import lax
from jax.experimental import pallas as pl
from jax.experimental.pallas import tpu as pltpu
from jax.sharding import PartitionSpec as P

HD = 64
WINDOW = 128
NZ, NY, NC, NX = 8, 4, 2, 4
PLANE = NY * NC
SP = NZ * PLANE
SPAN = 512
BLOCKS = SPAN // WINDOW
HEADS = 4
OUT_ROWS = HEADS * HD
OUT_HALF = OUT_ROWS // NC
PART = 1024
ROWS = 128
HALF = 64
CAP = 12
SLOTS = 2 * CAP
PACK = PLANE * SLOTS
D = 2048
FF = 512
EXPERTS = 64
MESH = pl.DeviceIdType.MESH
BF = jnp.bfloat16
F32 = jnp.float32

norm_eps = 1e-06


def dot(a, b):
    return jnp.dot(a, b, preferred_element_type=F32)


def silu(v):
    return v / (1.0 + jnp.exp(-v))


def chunk_of(delta):
    return 0 if delta == 0 else (2 * delta - 1 if delta <= NZ // 2 else 2 * (NZ - delta))


NEAR = 6
ROUTES = tuple((2 * n + turn, step, turn) for n, step in enumerate((0, 1, -1, 0)) for turn in range(NC))


def layer_kernel(
    q, k, v, docs, sink, wout, residual, gain, ids, weight, eg, eu, ed, shg, shu, shd, out,
    qv, ekv, edoc, attn, atf, wo, resid,
    tok, tx, rx, ret, rst, rsx, info, inf, wg, wu, wd, vg, vu, vd, sg, su, sd, sacc, hid,
    h_s, h_r, a_s, a_r, o_s, o_r, f_s, f_r,
    z_s, z_r, i_s, i_r, d_s, d_r, e_s, e_r, p_s, p_r, x_s, x_r, t_s, t_r, q_s, q_r, u_s, u_r, w_s,
):
    sp, x = lax.axis_index("sp"), lax.axis_index("tp")
    z, mine = sp // PLANE, sp % PLANE
    core = sp % NC
    twin = (sp + 1 - 2 * core, x)

    def at_sp(step):
        return ((sp + step) % SP, x)

    def at_z(dz):
        return ((z + dz) % NZ * PLANE + mine, x)

    def at_plane(j):
        return (z * PLANE + j, x)

    def at_x(dx):
        return (sp, (x + dx) % NX)

    def plane_of(dy, turn):
        return (mine // NC + dy + NY) % NY * NC + (core + turn) % NC

    def send(src, dst, ssem, rsem, device):
        copy = pltpu.make_async_remote_copy(
            src_ref=src, dst_ref=dst, send_sem=ssem, recv_sem=rsem, device_id=device, device_id_type=MESH
        )
        copy.start()

    def landed(ref, sem):
        pltpu.make_async_copy(ref, ref, sem).wait()

    local = [
        pltpu.make_async_copy(q, qv, w_s.at[0]),
        pltpu.make_async_copy(residual, resid, w_s.at[1]),
        pltpu.make_async_copy(wout, wo.at[0], w_s.at[2]),
        pltpu.make_async_copy(shg, sg.at[0], w_s.at[3]),
        pltpu.make_async_copy(shu, su.at[0], w_s.at[4]),
        pltpu.make_async_copy(shd, sd.at[0], w_s.at[5]),
        pltpu.make_async_copy(eg.at[0], wg, w_s.at[6]),
        pltpu.make_async_copy(eu.at[0], wu, w_s.at[7]),
        pltpu.make_async_copy(ed.at[0], wd, w_s.at[8]),
    ]
    for copy in local[:2]:
        copy.start()

    barrier = pltpu.get_barrier_semaphore()
    peers = [at_z(dz) for dz in range(1, NZ)] + [at_x(dx) for dx in range(1, NX)]
    peers += [at_plane((mine + off) % PLANE) for off in range(1, PLANE)]
    peers += [at_sp(1), at_sp(SP - 1)]
    for device in peers:
        pl.semaphore_signal(barrier, inc=1, device_id=device, device_id_type=MESH)

    ekv[0:HD, pl.ds(WINDOW, SPAN)] = k[...]
    ekv[HD : 2 * HD, pl.ds(WINDOW, SPAN)] = v[...]
    for b in range(BLOCKS):
        edoc[b + 1] = jnp.broadcast_to(docs[b : b + 1, :].astype(F32), (8, ROWS))

    far = (vg, vu, vd)

    def quarter(a, step):
        rows = far[a].shape[0] // NX
        return pl.ds(pl.multiple_of((x + step) % NX * rows, rows), rows)

    def eighth(a, step, k):
        rows = far[a].shape[0] // NX
        return pl.ds(pl.multiple_of((x + step) % NX * rows + k * (rows // 2), rows // 2), rows // 2)

    def unit(k):
        return (0 if k == 3 else k, eighth(0, 0, k // 3) if k % 3 == 0 else quarter(k, 0))

    def far_fetch(k):
        a, rows = unit(k)
        send((eg, eu, ed)[a].at[0, rows], far[a].at[rows], q_s.at[k], q_r.at[k], at_plane((mine + PLANE // 2) % PLANE))

    def far_start(k):
        a, rows = unit(k)
        own = far[a].at[rows]
        landed(own, q_r.at[k])
        send(own, own, u_s.at[k, 1], u_r.at[k, 1], at_x(1))
        send(own, own, u_s.at[k, 3], u_r.at[k, 3], at_x(3))

    def far_relay(a):
        if a == 0:
            landed(far[0].at[eighth(0, 3, 0)], u_r.at[0, 1])
            landed(far[0].at[eighth(0, 3, 1)], u_r.at[3, 1])
        else:
            landed(far[a].at[quarter(a, 3)], u_r.at[a, 1])
        half = far[a].at[eighth(a, 3, 0)]
        send(half, half, u_s.at[a, 0], u_r.at[a, 0], at_x(1))
        if a == 0:
            landed(far[0].at[eighth(0, 1, 0)], u_r.at[0, 3])
            landed(far[0].at[eighth(0, 1, 1)], u_r.at[3, 3])
        else:
            landed(far[a].at[quarter(a, 1)], u_r.at[a, 3])
        half = far[a].at[eighth(a, 1, 1)]
        send(half, half, u_s.at[a, 2], u_r.at[a, 2], at_x(3))

    def far_end(a):
        landed(far[a].at[eighth(a, 2, 0)], u_r.at[a, 0])
        landed(far[a].at[eighth(a, 2, 1)], u_r.at[a, 2])

    pl.semaphore_wait(barrier, len(peers))
    send(ekv.at[:, pl.ds(WINDOW, WINDOW)], ekv.at[:, pl.ds(WINDOW + SPAN, WINDOW)], h_s.at[0], h_r.at[0], at_sp(SP - 1))
    send(edoc.at[1], edoc.at[BLOCKS + 1], h_s.at[1], h_r.at[1], at_sp(SP - 1))
    send(ekv.at[:, pl.ds(SPAN, WINDOW)], ekv.at[:, pl.ds(0, WINDOW)], h_s.at[2], h_r.at[2], at_sp(1))
    send(edoc.at[BLOCKS], edoc.at[0], h_s.at[3], h_r.at[3], at_sp(1))
    direct = pl.ds(pl.multiple_of(core * OUT_HALF, OUT_HALF), OUT_HALF)
    rest = pl.ds(pl.multiple_of((1 - core) * OUT_HALF, OUT_HALF), OUT_HALF)
    others = pl.ds(1, NX - 1)
    for dx in (1, 3, 2):
        send(wout.at[direct], wo.at[dx, direct], o_s.at[dx], o_r.at[dx], at_x(dx))

    expert = lax.broadcasted_iota(jnp.int32, (EXPERTS, ROWS), 0)
    hits = jnp.zeros((EXPERTS, ROWS), F32)
    wide = jnp.zeros((EXPERTS, ROWS), F32)
    for k in range(ids.shape[0]):
        named = ids[k : k + 1, :] == expert
        hits = hits + named.astype(F32)
        wide = wide + jnp.where(named, weight[k : k + 1, :], 0.0)
    row = lax.broadcasted_iota(jnp.int32, (ROWS, ROWS), 0)
    col = lax.broadcasted_iota(jnp.int32, (ROWS, ROWS), 1)
    earlier = ((row < col) & (row // HALF == col // HALF)).astype(BF)
    rank = dot(hits.astype(BF), earlier)
    half = lax.broadcasted_iota(jnp.int32, (EXPERTS, ROWS), 1) // HALF
    place = jnp.where(hits > 0.0, rank + (half * CAP).astype(F32), -1.0)
    for plane in range(NZ):
        lower = plane * PLANE
        info[plane, 0:PLANE, :] = place[lower : lower + PLANE]
        info[plane, PLANE : 2 * PLANE, :] = wide[lower : lower + PLANE]
    inf[0] = info[z]

    def attention(n, carry):
        b = jnp.where(n < 3, (n + 1) % 3, 3)

        @pl.when(n == 2)
        def _():
            landed(ekv.at[:, pl.ds(WINDOW + SPAN, WINDOW)], h_r.at[0])
            landed(edoc.at[BLOCKS + 1], h_r.at[1])
            landed(ekv.at[:, pl.ds(0, WINDOW)], h_r.at[2])
            landed(edoc.at[0], h_r.at[3])

            @pl.when(sp == 0)
            def _():
                edoc[0] = jnp.full((8, ROWS), -1.0, F32)

            @pl.when(sp == SP - 1)
            def _():
                edoc[BLOCKS + 1] = jnp.full((8, ROWS), -1.0, F32)

        rows = pl.ds(pl.multiple_of(b * WINDOW, WINDOW), WINDOW)
        band = ekv[:, pl.ds(pl.multiple_of(b * WINDOW, WINDOW), 3 * WINDOW)]
        own_doc = jnp.broadcast_to(edoc[b + 1][0:1, :], (WINDOW, WINDOW)).T
        at_row = lax.broadcasted_iota(jnp.int32, (WINDOW, WINDOW), 0)
        at_col = lax.broadcasted_iota(jnp.int32, (WINDOW, WINDOW), 1)
        near = (at_col >= at_row, at_row >= 0, at_col <= at_row)
        allowed = jnp.concatenate(
            [
                ((own_doc == edoc[b + t][0:1, :]) & near[t]).astype(F32)
                for t in range(3)
            ],
            axis=1,
        )
        heads = []
        for h in range(HEADS):
            query = qv[rows, h * HD : (h + 1) * HD]
            scores = dot(query, band[:HD]) * HD ** (-0.5)
            scores = jnp.where(allowed > 0.0, scores, -jnp.inf)
            row_max = jnp.maximum(jnp.max(scores, axis=1, keepdims=True), sink[h])
            grown = jnp.exp(scores - row_max)
            total = jnp.sum(grown, axis=1, keepdims=True) + jnp.exp(sink[h] - row_max)
            probs = (grown / total).astype(BF)
            mixed = lax.dot_general(probs, band[HD:], (((1,), (1,)), ((), ())), preferred_element_type=F32)
            heads.append(mixed.astype(BF))
        attn[b] = jnp.concatenate(heads, axis=1)
        slot = (b + NX - x) % NX

        @pl.when(b != x)
        def _():
            send(attn.at[b], atf.at[slot], a_s.at[slot], a_r.at[slot], (sp, b))

        @pl.when(b == x)
        def _():
            pltpu.make_async_copy(attn.at[b], atf.at[0], a_r.at[0]).start()

        return carry

    local[0].wait()
    lax.fori_loop(0, BLOCKS, attention, 0)

    for copy in local[2:]:
        copy.start()
    for k in (0, 3, 1, 2):
        far_fetch(k)
    for dx in (1, 3, 2):
        landed(wo.at[dx, direct], o_r.at[dx])
        send(wo.at[dx, direct], wo.at[dx, direct], f_s.at[dx], f_r.at[dx], twin)
    local[1].wait()
    local[2].wait()
    for dx in range(NX):
        landed(atf.at[dx], a_r.at[dx])
    for dx in range(1, NX):
        landed(wo.at[dx, rest], f_r.at[dx])

    far_start(0)

    def project(n, squares):
        cols = pl.ds(pl.multiple_of(n * 256, 256), 256)
        mixed = dot(atf[0], wo[0, :, cols])
        for dx in range(1, NX):
            mixed = mixed + dot(atf[dx], wo[dx, :, cols])
        rounded = (resid[:, cols].astype(F32) + mixed).astype(BF)
        resid[:, cols] = rounded
        squared = rounded.astype(F32)
        squared = squared * squared
        return squares + squared[:, :128] + squared[:, 128:]

    squares = lax.fori_loop(0, D // 256, project, jnp.zeros((ROWS, 128), F32))
    scale = lax.rsqrt(jnp.sum(squares, axis=1, keepdims=True) * (1.0 / D) + norm_eps)
    for h in range(2):
        cols = pl.ds(h * PART, PART)
        tok[0, h] = (resid[:, cols].astype(F32) * scale * gain[:, cols]).astype(BF)

    for delta in range(1, NZ):
        i = chunk_of(delta)
        send(info.at[(z + delta) % NZ], inf.at[i], i_s.at[i], i_r.at[i], at_z(delta))
    for h in range(2):
        send(tok.at[0, h], tok.at[1, h], z_s.at[1, h], z_r.at[1, h], at_z(1))
        send(tok.at[0, h], tok.at[2, h], z_s.at[2, h], z_r.at[2, h], at_z(NZ - 1))

    def placed(i):
        slot = lax.broadcasted_iota(jnp.int32, (PLANE, SLOTS, ROWS), 1).astype(F32)
        return (inf[i, 0:PLANE, :][:, None, :] == slot).astype(F32)

    def forward(i, h):
        landed(tok.at[i, h], z_r.at[i, h])

        @pl.when(h == 0)
        def _():
            landed(inf.at[i], i_r.at[i])

        @pl.when((i < 5) | ((i == 5) & (h == 0)) | ((i == 6) & (h == 1)))
        def _():
            way = 1 + (NZ - 2) * ((i + 1) % 2)
            to = jnp.minimum(i + 2, NZ - 1)
            send(tok.at[i, h], tok.at[to, h], z_s.at[to, h], z_r.at[to, h], at_z(way))

    def pack(i, h):
        pick = placed(i).reshape(PACK, ROWS).astype(BF)
        for n in range(PART // 512):
            cols = pl.ds(n * 512, 512)
            tx[i, h, :, :, cols] = dot(pick, tok[i, h, :, cols]).astype(BF).reshape(PLANE, SLOTS, 512)
        for slot, step, turn in ROUTES:
            runner = plane_of(-step, turn)
            expert = plane_of(2, turn) if slot >= NEAR else runner
            if step == 0 and turn == 0:
                pltpu.make_async_copy(tx.at[i, h, expert], rx.at[i, h, slot], d_r.at[i]).start()
            else:
                send(tx.at[i, h, expert], rx.at[i, h, slot], d_s.at[i], d_r.at[i], at_plane(runner))

    def run_expert(i, lower, count, gate_w, up_w, down_w):
        rows, slots = count * SLOTS, pl.ds(lower, count)

        def hidden_tile(n, carry):
            cols = pl.ds(pl.multiple_of(n * 256, 256), 256)
            left, right = rx[i, 0, slots].reshape(rows, PART), rx[i, 1, slots].reshape(rows, PART)
            gate = dot(left, gate_w[0:PART, cols]) + dot(right, gate_w[PART:D, cols])
            up = dot(left, up_w[0:PART, cols]) + dot(right, up_w[PART:D, cols])
            hid[0:rows, cols] = (silu(gate) * up).astype(BF)
            return carry

        lax.fori_loop(0, FF // 256, hidden_tile, 0)

        def out_tile(n, carry):
            cols = pl.ds(pl.multiple_of(n * 512, 512), 512)
            made = dot(hid[0:rows, :], down_w[:, cols]).astype(BF).reshape(count, SLOTS, 512)
            rx[i, n // 2, slots, :, pl.ds(pl.multiple_of(n % 2 * 512, 512), 512)] = made
            return carry

        lax.fori_loop(0, D // 512, out_tile, 0)

    def give_back(i, routes):
        for h in range(2):
            for slot, step, turn in routes:
                source = plane_of(step, turn)
                expert = plane_of(2, 0) if slot >= NEAR else mine
                if step == 0 and turn == 0:
                    pltpu.make_async_copy(rx.at[i, h, slot], ret.at[i, h, expert], e_r.at[i, h]).start()
                else:
                    send(rx.at[i, h, slot], ret.at[i, h, expert], e_s.at[i, h], e_r.at[i, h], at_plane(source))

    def run_near(i):
        landed(rx.at[i], d_r.at[i])
        run_expert(i, 0, NEAR, wg, wu, wd)

    def run_far(i):
        run_expert(i, NEAR, PLANE - NEAR, vg, vu, vd)
        give_back(i, ROUTES[NEAR:])

    def pieces(n, carry):
        i = 1 + n // 4 * 2 + n % 2
        h = n % 4 // 2

        @pl.when(i < NZ)
        def _():
            forward(i, h)

            @pl.when(i >= 3)
            def _():
                pack(i, h)

        for at, task in (
            (1, lambda: far_start(2)),
            (3, lambda: far_relay(0)),
            (7, lambda: far_relay(1)),
            (11, lambda: far_relay(2)),
            (12, shared_start),
        ):
            pl.when(n == at)(task)

        @pl.when((n == 9) | (n == 11))
        def _():
            run_near((n - 3) // 2)

        return carry

    shared = ((shg, sg), (shu, su), (shd, sd))

    def twin_half(a, which):
        rows = shared[a][0].shape[0] // NC
        return pl.ds(pl.multiple_of(which * rows, rows), rows)

    def shared_start():
        for copy in local[3:6]:
            copy.wait()
        for dx in (1, 3, 2):
            for a, (mat, full) in enumerate(shared):
                rows = twin_half(a, core)
                send(full.at[0, rows], full.at[dx, rows], x_s.at[a, dx], x_r.at[a, dx], at_x(dx))

    def shared_relay():
        for a, (_, full) in enumerate(shared):
            rows = twin_half(a, core)
            for dx in (1, 3, 2):
                landed(full.at[dx, rows], x_r.at[a, dx])
            send(full.at[others, rows], full.at[others, rows], t_s.at[a], t_r.at[a], twin)

    far_start(3)
    far_start(1)
    for copy in local[6:]:
        copy.wait()
    lax.fori_loop(0, 2 * NZ - 1, pieces, 0)

    near_routes = ROUTES[:NEAR]
    run_near(5)
    run_near(6)
    give_back(6, near_routes)
    run_near(7)
    give_back(7, near_routes)
    give_back(5, near_routes)
    for a in range(3):
        far_end(a)
    run_far(7)

    def nearest(n, carry):
        pack((n // 2 + 1) % 3, n % 2)

        @pl.when(n == 3)
        def _():
            give_back(4, near_routes)
            give_back(3, near_routes)

        return carry

    lax.fori_loop(0, 6, nearest, 0)
    run_far(6)

    def combined(i):
        scaled = placed(i) * inf[i, PLANE : 2 * PLANE, :][:, None, :]
        scaled = jnp.concatenate([scaled.reshape(PACK, ROWS), jnp.zeros((256 - PACK, ROWS), F32)], axis=0)
        scaled = scaled.T[:, :PACK]
        high = scaled.astype(BF)
        low = (scaled - high.astype(F32)).astype(BF)

        def part(h, cols):
            rows = ret[i, h, :, :, cols].reshape(PACK, 512)
            return dot(high, rows) + dot(low, rows)

        return part

    def pass_on(i, h, way):
        send(rst.at[i, h], rsx.at[i, h], p_s.at[i, h], p_r.at[i, h], at_z(way))

    def reduce_chunk(i, ways, arrives):
        part = combined(i)
        for h in range(2):
            landed(ret.at[i, h], e_r.at[i, h])
            source = arrives[h]
            if source is not None:
                landed(rsx.at[source, h], p_r.at[source, h])
            for n in range(PART // 512):
                cols = pl.ds(n * 512, 512)
                total = part(h, cols)
                if source is not None:
                    total = total + rsx[source, h, :, cols].astype(F32)
                rst[i, h, :, cols] = total.astype(BF)
            pass_on(i, h, ways[h])

    reduce_chunk(7, (NZ - 1, 1), (None, None))
    run_far(5)
    reduce_chunk(6, (1, 1), (None, 7))
    reduce_chunk(5, (NZ - 1, NZ - 1), (7, None))

    def middle(n, carry):
        run_far(4 - n)
        run_near(2 - n)
        give_back(2 - n, near_routes)
        return carry

    lax.fori_loop(0, 2, middle, 0)

    def nearer(n, carry):
        i = 4 - n
        way = 1 + (NZ - 2) * (i % 2)

        @pl.when(n == 2)
        def _():
            run_near(0)
            give_back(0, near_routes)
            run_far(2)

        reduce_chunk(i, (way, way), (i + 2, i + 2))

        @pl.when(n >= 2)
        def _():
            run_far(3 - n)

        pl.when(n == 2)(shared_relay)
        return carry

    lax.fori_loop(0, 4, nearer, 0)

    for a, (_, full) in enumerate(shared):
        landed(full.at[others, twin_half(a, 1 - core)], t_r.at[a])
    sacc[...] = jnp.zeros_like(sacc)

    def shared_block(dx, carry):
        left, right = tok[0, 0], tok[0, 1]
        gate = dot(left, sg[dx, 0:PART]) + dot(right, sg[dx, PART:D])
        up = dot(left, su[dx, 0:PART]) + dot(right, su[dx, PART:D])
        units = (silu(gate) * up).astype(BF)
        for n in range(D // 512):
            cols = pl.ds(n * 512, 512)
            sacc[:, cols] = sacc[:, cols] + dot(units, sd[dx, :, cols])
        return carry

    lax.fori_loop(0, NX, shared_block, 0)

    part = combined(0)
    for h in range(2):
        landed(ret.at[0, h], e_r.at[0, h])
        landed(rsx.at[2, h], p_r.at[2, h])
        landed(rsx.at[1, h], p_r.at[1, h])
        for n in range(PART // 512):
            cols, wide = pl.ds(n * 512, 512), pl.ds(h * PART + n * 512, 512)
            routed = part(h, cols) + rsx[2, h, :, cols].astype(F32) + rsx[1, h, :, cols].astype(F32)
            out[:, wide] = (resid[:, wide].astype(F32) + sacc[:, wide] + routed).astype(BF)

    for i in range(NZ):
        landed(tx.at[i, :, pl.ds(0, PLANE - 2)], d_s.at[i])
        if i > 0:
            landed(info.at[i], i_s.at[i])
        for h in range(2):
            landed(rx.at[i, h, pl.ds(0, PLANE - 2)], e_s.at[i, h])
            if i > 0:
                landed(tok.at[i, h], z_s.at[i, h])
                landed(rst.at[i, h], p_s.at[i, h])
    landed(ekv.at[:, pl.ds(0, WINDOW)], h_s.at[0])
    landed(edoc.at[0], h_s.at[1])
    landed(ekv.at[:, pl.ds(0, WINDOW)], h_s.at[2])
    landed(edoc.at[0], h_s.at[3])
    for dx in range(1, NX):
        landed(atf.at[0], a_s.at[dx])
        landed(wo.at[0, direct], o_s.at[dx])
        landed(wo.at[0, direct], f_s.at[dx])
        for a, (_, full) in enumerate(shared):
            landed(full.at[0, twin_half(a, core)], x_s.at[a, dx])
    for a, (_, full) in enumerate(shared):
        landed(full.at[others, twin_half(a, core)], t_s.at[a])
        landed(far[a].at[eighth(a, 0, 0)], u_s.at[a, 0])
        landed(far[a].at[eighth(a, 0, 0)], u_s.at[a, 2])
    for k in range(4):
        a, rows = unit(k)
        landed(far[a].at[rows], q_s.at[k])
        landed(far[a].at[rows], u_s.at[k, 1])
        landed(far[a].at[rows], u_s.at[k, 3])


def shards(
    queries,
    keys,
    values,
    doc_ids,
    sink_logit,
    w_out,
    residual,
    ffn_gain,
    expert_ids,
    expert_weight,
    exp_gate,
    exp_up,
    exp_down,
    shared_gate,
    shared_up,
    shared_down,
):
    vmem = pl.BlockSpec(memory_space=pltpu.VMEM)
    smem = pl.BlockSpec(memory_space=pltpu.SMEM)
    hbm = pl.BlockSpec(memory_space=pl.ANY)
    dma = pltpu.SemaphoreType.DMA
    unit = FF // NX
    return pl.pallas_call(
        layer_kernel,
        out_shape=jax.ShapeDtypeStruct((ROWS, D), BF),
        in_specs=[hbm, vmem, vmem, vmem, smem, hbm, hbm, vmem, vmem, vmem] + [hbm] * 6,
        out_specs=vmem,
        scratch_shapes=[
            pltpu.VMEM((SPAN, HEADS * HD), BF),
            pltpu.VMEM((2 * HD, SPAN + 2 * WINDOW), BF),
            pltpu.VMEM((BLOCKS + 2, 8, ROWS), F32),
            pltpu.VMEM((BLOCKS, ROWS, HEADS * HD), BF),
            pltpu.VMEM((NX, ROWS, HEADS * HD), BF),
            pltpu.VMEM((NX, OUT_ROWS, D), BF),
            pltpu.VMEM((ROWS, D), BF),
            pltpu.VMEM((NZ, 2, ROWS, PART), BF),
            pltpu.VMEM((NZ, 2, PLANE, SLOTS, PART), BF),
            pltpu.VMEM((NZ, 2, PLANE, SLOTS, PART), BF),
            pltpu.VMEM((NZ, 2, PLANE, SLOTS, PART), BF),
            pltpu.VMEM((NZ, 2, ROWS, PART), BF),
            pltpu.VMEM((NZ, 2, ROWS, PART), BF),
            pltpu.VMEM((NZ, 2 * PLANE, ROWS), F32),
            pltpu.VMEM((NZ, 2 * PLANE, ROWS), F32),
            pltpu.VMEM((D, FF), BF),
            pltpu.VMEM((D, FF), BF),
            pltpu.VMEM((FF, D), BF),
            pltpu.VMEM((D, FF), BF),
            pltpu.VMEM((D, FF), BF),
            pltpu.VMEM((FF, D), BF),
            pltpu.VMEM((NX, D, unit), BF),
            pltpu.VMEM((NX, D, unit), BF),
            pltpu.VMEM((NX, unit, D), BF),
            pltpu.VMEM((ROWS, D), F32),
            pltpu.VMEM((PACK, FF), BF),
        ]
        + [dma((4,))] * 8
        + [dma((NZ, 2))] * 2
        + [dma((NZ,))] * 4
        + [dma((NZ, 2))] * 4
        + [dma((3, NX))] * 2
        + [dma((3,))] * 2
        + [dma((4,))] * 2
        + [dma((4, NX))] * 2
        + [dma((9,))],
        compiler_params=pltpu.CompilerParams(
            collective_id=1, has_side_effects=True, vmem_limit_bytes=62 * 2**20
        ),
        name="layer",
    )(
        queries, keys.T, values.T, doc_ids.reshape(BLOCKS, ROWS), sink_logit, w_out, residual,
        ffn_gain.reshape(1, D), expert_ids.T, expert_weight.T,
        exp_gate, exp_up, exp_down, shared_gate, shared_up, shared_down,
    )


def solution(mesh):
    placed = (
        P("sp", "tp"),
        P("sp", "tp"),
        P("sp", "tp"),
        P("sp"),
        P("tp"),
        P("tp", None),
        P(("sp", "tp"), None),
        P(),
        P(("sp", "tp"), None),
        P(("sp", "tp"), None),
        P("sp", None, None),
        P("sp", None, None),
        P("sp", None, None),
        P(None, "tp"),
        P(None, "tp"),
        P("tp", None),
    )
    return jax.shard_map(
        shards, mesh=mesh, in_specs=placed, out_specs=P(("sp", "tp"), None), check_vma=False
    )
```

```python
import functools

import jax
import jax.numpy as jnp
from jax import lax
from jax.experimental import pallas as pl
from jax.experimental.pallas import tpu as pltpu
from jax.sharding import PartitionSpec as P

HD = 64
WINDOW = 128
NZ, NY, NC, NX = 8, 4, 2, 4
PLANE = NY * NC
SP = NZ * PLANE
SPAN = 512
BLOCKS = SPAN // WINDOW
HEADS = 4
OUT_ROWS = HEADS * HD
OUT_HALF = OUT_ROWS // NC
PART = 1024
ROWS = 128
HALF = 64
CAP = 12
SLOTS = 2 * CAP
PACK = PLANE * SLOTS
D = 2048
FF = 512
EXPERTS = 64
MESH = pl.DeviceIdType.MESH
BF = jnp.bfloat16
F32 = jnp.float32

norm_eps = 1e-06


def dot(a, b):
    return jnp.dot(a, b, preferred_element_type=F32)


def silu(v):
    return v / (1.0 + jnp.exp(-v))


def chunk_of(delta):
    return 0 if delta == 0 else (2 * delta - 1 if delta <= NZ // 2 else 2 * (NZ - delta))


NEAR = 6
ROUTES = tuple((2 * n + turn, step, turn) for n, step in enumerate((0, 1, -1, 0)) for turn in range(NC))


def layer_kernel(
    q, k, v, docs, sink, wout, residual, gain, ids, weight, eg, eu, ed, shg, shu, shd, out,
    qv, ekv, edoc, attn, atf, wo, resid,
    tok, tx, rx, ret, rst, rsx, info, inf, wg, wu, wd, vg, vu, vd, sg, su, sd, sacc, hid,
    h_s, h_r, a_s, a_r, o_s, o_r, f_s, f_r,
    z_s, z_r, i_s, i_r, d_s, d_r, e_s, e_r, p_s, p_r, x_s, x_r, t_s, t_r, q_s, q_r, u_s, u_r, w_s,
):
    sp, x = lax.axis_index("sp"), lax.axis_index("tp")
    z, mine = sp // PLANE, sp % PLANE
    core = sp % NC
    twin = (sp + 1 - 2 * core, x)

    def at_sp(step):
        return ((sp + step) % SP, x)

    def at_z(dz):
        return ((z + dz) % NZ * PLANE + mine, x)

    def at_plane(j):
        return (z * PLANE + j, x)

    def at_x(dx):
        return (sp, (x + dx) % NX)

    def plane_of(dy, turn):
        return (mine // NC + dy + NY) % NY * NC + (core + turn) % NC

    def send(src, dst, ssem, rsem, device):
        copy = pltpu.make_async_remote_copy(
            src_ref=src, dst_ref=dst, send_sem=ssem, recv_sem=rsem, device_id=device, device_id_type=MESH
        )
        copy.start()

    def landed(ref, sem):
        pltpu.make_async_copy(ref, ref, sem).wait()

    local = [
        pltpu.make_async_copy(q, qv, w_s.at[0]),
        pltpu.make_async_copy(residual, resid, w_s.at[1]),
        pltpu.make_async_copy(wout, wo.at[0], w_s.at[2]),
        pltpu.make_async_copy(shg, sg.at[0], w_s.at[3]),
        pltpu.make_async_copy(shu, su.at[0], w_s.at[4]),
        pltpu.make_async_copy(shd, sd.at[0], w_s.at[5]),
        pltpu.make_async_copy(eg.at[0], wg, w_s.at[6]),
        pltpu.make_async_copy(eu.at[0], wu, w_s.at[7]),
        pltpu.make_async_copy(ed.at[0], wd, w_s.at[8]),
    ]
    for copy in local[:2]:
        copy.start()

    barrier = pltpu.get_barrier_semaphore()
    peers = [at_z(dz) for dz in range(1, NZ)] + [at_x(dx) for dx in range(1, NX)]
    peers += [at_plane((mine + off) % PLANE) for off in range(1, PLANE)]
    peers += [at_sp(1), at_sp(SP - 1)]
    for device in peers:
        pl.semaphore_signal(barrier, inc=1, device_id=device, device_id_type=MESH)

    ekv[0:HD, pl.ds(WINDOW, SPAN)] = k[...]
    ekv[HD : 2 * HD, pl.ds(WINDOW, SPAN)] = v[...]
    for b in range(BLOCKS):
        edoc[b + 1] = jnp.broadcast_to(docs[b : b + 1, :].astype(F32), (8, ROWS))

    far = (vg, vu, vd)

    def quarter(a, step):
        rows = far[a].shape[0] // NX
        return pl.ds(pl.multiple_of((x + step) % NX * rows, rows), rows)

    def eighth(a, step, k):
        rows = far[a].shape[0] // NX
        return pl.ds(pl.multiple_of((x + step) % NX * rows + k * (rows // 2), rows // 2), rows // 2)

    def unit(k):
        return (0 if k == 3 else k, eighth(0, 0, k // 3) if k % 3 == 0 else quarter(k, 0))

    def far_fetch(k):
        a, rows = unit(k)
        send((eg, eu, ed)[a].at[0, rows], far[a].at[rows], q_s.at[k], q_r.at[k], at_plane((mine + PLANE // 2) % PLANE))

    def far_start(k):
        a, rows = unit(k)
        own = far[a].at[rows]
        landed(own, q_r.at[k])
        send(own, own, u_s.at[k, 1], u_r.at[k, 1], at_x(1))
        send(own, own, u_s.at[k, 3], u_r.at[k, 3], at_x(3))

    def far_relay(a):
        if a == 0:
            landed(far[0].at[eighth(0, 3, 0)], u_r.at[0, 1])
            landed(far[0].at[eighth(0, 3, 1)], u_r.at[3, 1])
        else:
            landed(far[a].at[quarter(a, 3)], u_r.at[a, 1])
        half = far[a].at[eighth(a, 3, 0)]
        send(half, half, u_s.at[a, 0], u_r.at[a, 0], at_x(1))
        if a == 0:
            landed(far[0].at[eighth(0, 1, 0)], u_r.at[0, 3])
            landed(far[0].at[eighth(0, 1, 1)], u_r.at[3, 3])
        else:
            landed(far[a].at[quarter(a, 1)], u_r.at[a, 3])
        half = far[a].at[eighth(a, 1, 1)]
        send(half, half, u_s.at[a, 2], u_r.at[a, 2], at_x(3))

    def far_end(a):
        landed(far[a].at[eighth(a, 2, 0)], u_r.at[a, 0])
        landed(far[a].at[eighth(a, 2, 1)], u_r.at[a, 2])

    pl.semaphore_wait(barrier, len(peers))
    send(ekv.at[:, pl.ds(WINDOW, WINDOW)], ekv.at[:, pl.ds(WINDOW + SPAN, WINDOW)], h_s.at[0], h_r.at[0], at_sp(SP - 1))
    send(edoc.at[1], edoc.at[BLOCKS + 1], h_s.at[1], h_r.at[1], at_sp(SP - 1))
    send(ekv.at[:, pl.ds(SPAN, WINDOW)], ekv.at[:, pl.ds(0, WINDOW)], h_s.at[2], h_r.at[2], at_sp(1))
    send(edoc.at[BLOCKS], edoc.at[0], h_s.at[3], h_r.at[3], at_sp(1))
    direct = pl.ds(pl.multiple_of(core * OUT_HALF, OUT_HALF), OUT_HALF)
    rest = pl.ds(pl.multiple_of((1 - core) * OUT_HALF, OUT_HALF), OUT_HALF)
    others = pl.ds(1, NX - 1)
    for dx in (1, 3, 2):
        send(wout.at[direct], wo.at[dx, direct], o_s.at[dx], o_r.at[dx], at_x(dx))

    expert = lax.broadcasted_iota(jnp.int32, (EXPERTS, ROWS), 0)
    hits = jnp.zeros((EXPERTS, ROWS), F32)
    wide = jnp.zeros((EXPERTS, ROWS), F32)
    for k in range(ids.shape[0]):
        named = ids[k : k + 1, :] == expert
        hits = hits + named.astype(F32)
        wide = wide + jnp.where(named, weight[k : k + 1, :], 0.0)
    row = lax.broadcasted_iota(jnp.int32, (ROWS, ROWS), 0)
    col = lax.broadcasted_iota(jnp.int32, (ROWS, ROWS), 1)
    earlier = ((row < col) & (row // HALF == col // HALF)).astype(BF)
    rank = dot(hits.astype(BF), earlier)
    half = lax.broadcasted_iota(jnp.int32, (EXPERTS, ROWS), 1) // HALF
    place = jnp.where(hits > 0.0, rank + (half * CAP).astype(F32), -1.0)
    for plane in range(NZ):
        lower = plane * PLANE
        info[plane, 0:PLANE, :] = place[lower : lower + PLANE]
        info[plane, PLANE : 2 * PLANE, :] = wide[lower : lower + PLANE]
    inf[0] = info[z]

    def attention(n, carry):
        b = jnp.where(n < 3, (n + 1) % 3, 3)

        @pl.when(n == 2)
        def _():
            landed(ekv.at[:, pl.ds(WINDOW + SPAN, WINDOW)], h_r.at[0])
            landed(edoc.at[BLOCKS + 1], h_r.at[1])
            landed(ekv.at[:, pl.ds(0, WINDOW)], h_r.at[2])
            landed(edoc.at[0], h_r.at[3])

            @pl.when(sp == 0)
            def _():
                edoc[0] = jnp.full((8, ROWS), -1.0, F32)

            @pl.when(sp == SP - 1)
            def _():
                edoc[BLOCKS + 1] = jnp.full((8, ROWS), -1.0, F32)

        rows = pl.ds(pl.multiple_of(b * WINDOW, WINDOW), WINDOW)
        band = ekv[:, pl.ds(pl.multiple_of(b * WINDOW, WINDOW), 3 * WINDOW)]
        own_doc = jnp.broadcast_to(edoc[b + 1][0:1, :], (WINDOW, WINDOW)).T
        at_row = lax.broadcasted_iota(jnp.int32, (WINDOW, WINDOW), 0)
        at_col = lax.broadcasted_iota(jnp.int32, (WINDOW, WINDOW), 1)
        near = (at_col >= at_row, at_row >= 0, at_col <= at_row)
        allowed = jnp.concatenate(
            [
                ((own_doc == edoc[b + t][0:1, :]) & near[t]).astype(F32)
                for t in range(3)
            ],
            axis=1,
        )
        heads = []
        for h in range(HEADS):
            query = qv[rows, h * HD : (h + 1) * HD]
            scores = dot(query, band[:HD]) * HD ** (-0.5)
            scores = jnp.where(allowed > 0.0, scores, -jnp.inf)
            row_max = jnp.maximum(jnp.max(scores, axis=1, keepdims=True), sink[h])
            grown = jnp.exp(scores - row_max)
            total = jnp.sum(grown, axis=1, keepdims=True) + jnp.exp(sink[h] - row_max)
            probs = (grown / total).astype(BF)
            mixed = lax.dot_general(probs, band[HD:], (((1,), (1,)), ((), ())), preferred_element_type=F32)
            heads.append(mixed.astype(BF))
        attn[b] = jnp.concatenate(heads, axis=1)
        slot = (b + NX - x) % NX

        @pl.when(b != x)
        def _():
            send(attn.at[b], atf.at[slot], a_s.at[slot], a_r.at[slot], (sp, b))

        @pl.when(b == x)
        def _():
            pltpu.make_async_copy(attn.at[b], atf.at[0], a_r.at[0]).start()

        return carry

    local[0].wait()
    lax.fori_loop(0, BLOCKS, attention, 0)

    for copy in local[2:]:
        copy.start()
    for k in (0, 3, 1, 2):
        far_fetch(k)
    for dx in (1, 3, 2):
        landed(wo.at[dx, direct], o_r.at[dx])
        send(wo.at[dx, direct], wo.at[dx, direct], f_s.at[dx], f_r.at[dx], twin)
    local[1].wait()
    local[2].wait()
    for dx in range(NX):
        landed(atf.at[dx], a_r.at[dx])
    for dx in range(1, NX):
        landed(wo.at[dx, rest], f_r.at[dx])

    far_start(0)

    def project(n, squares):
        cols = pl.ds(pl.multiple_of(n * 256, 256), 256)
        mixed = dot(atf[0], wo[0, :, cols])
        for dx in range(1, NX):
            mixed = mixed + dot(atf[dx], wo[dx, :, cols])
        rounded = (resid[:, cols].astype(F32) + mixed).astype(BF)
        resid[:, cols] = rounded
        squared = rounded.astype(F32)
        squared = squared * squared
        return squares + squared[:, :128] + squared[:, 128:]

    squares = lax.fori_loop(0, D // 256, project, jnp.zeros((ROWS, 128), F32))
    scale = lax.rsqrt(jnp.sum(squares, axis=1, keepdims=True) * (1.0 / D) + norm_eps)
    for h in range(2):
        cols = pl.ds(h * PART, PART)
        tok[0, h] = (resid[:, cols].astype(F32) * scale * gain[:, cols]).astype(BF)

    for delta in range(1, NZ):
        i = chunk_of(delta)
        send(info.at[(z + delta) % NZ], inf.at[i], i_s.at[i], i_r.at[i], at_z(delta))
    for h in range(2):
        send(tok.at[0, h], tok.at[1, h], z_s.at[1, h], z_r.at[1, h], at_z(1))
        send(tok.at[0, h], tok.at[2, h], z_s.at[2, h], z_r.at[2, h], at_z(NZ - 1))

    def placed(i):
        slot = lax.broadcasted_iota(jnp.int32, (PLANE, SLOTS, ROWS), 1).astype(F32)
        return (inf[i, 0:PLANE, :][:, None, :] == slot).astype(F32)

    def forward(i, h):
        landed(tok.at[i, h], z_r.at[i, h])

        @pl.when(h == 0)
        def _():
            landed(inf.at[i], i_r.at[i])

        @pl.when((i < 5) | ((i == 5) & (h == 0)) | ((i == 6) & (h == 1)))
        def _():
            way = 1 + (NZ - 2) * ((i + 1) % 2)
            to = jnp.minimum(i + 2, NZ - 1)
            send(tok.at[i, h], tok.at[to, h], z_s.at[to, h], z_r.at[to, h], at_z(way))

    def pack(i, h):
        pick = placed(i).reshape(PACK, ROWS).astype(BF)
        for n in range(PART // 512):
            cols = pl.ds(n * 512, 512)
            tx[i, h, :, :, cols] = dot(pick, tok[i, h, :, cols]).astype(BF).reshape(PLANE, SLOTS, 512)
        for slot, step, turn in ROUTES:
            runner = plane_of(-step, turn)
            expert = plane_of(2, turn) if slot >= NEAR else runner
            if step == 0 and turn == 0:
                pltpu.make_async_copy(tx.at[i, h, expert], rx.at[i, h, slot], d_r.at[i]).start()
            else:
                send(tx.at[i, h, expert], rx.at[i, h, slot], d_s.at[i], d_r.at[i], at_plane(runner))

    def run_expert(i, lower, count, gate_w, up_w, down_w):
        rows, slots = count * SLOTS, pl.ds(lower, count)

        def hidden_tile(n, carry):
            cols = pl.ds(pl.multiple_of(n * 256, 256), 256)
            left, right = rx[i, 0, slots].reshape(rows, PART), rx[i, 1, slots].reshape(rows, PART)
            gate = dot(left, gate_w[0:PART, cols]) + dot(right, gate_w[PART:D, cols])
            up = dot(left, up_w[0:PART, cols]) + dot(right, up_w[PART:D, cols])
            hid[0:rows, cols] = (silu(gate) * up).astype(BF)
            return carry

        lax.fori_loop(0, FF // 256, hidden_tile, 0)

        def out_tile(n, carry):
            cols = pl.ds(pl.multiple_of(n * 512, 512), 512)
            made = dot(hid[0:rows, :], down_w[:, cols]).astype(BF).reshape(count, SLOTS, 512)
            rx[i, n // 2, slots, :, pl.ds(pl.multiple_of(n % 2 * 512, 512), 512)] = made
            return carry

        lax.fori_loop(0, D // 512, out_tile, 0)

    def give_back(i, routes, halves=(0, 1)):
        for h in halves:
            for slot, step, turn in routes:
                source = plane_of(step, turn)
                expert = plane_of(2, 0) if slot >= NEAR else mine
                if step == 0 and turn == 0:
                    pltpu.make_async_copy(rx.at[i, h, slot], ret.at[i, h, expert], e_r.at[i, h]).start()
                else:
                    send(rx.at[i, h, slot], ret.at[i, h, expert], e_s.at[i, h], e_r.at[i, h], at_plane(source))

    def run_near(i):
        landed(rx.at[i], d_r.at[i])
        run_expert(i, 0, NEAR, wg, wu, wd)

    def run_far(i):
        run_expert(i, NEAR, PLANE - NEAR, vg, vu, vd)
        give_back(i, ROUTES[NEAR:])

    def pieces(n, carry):
        i = 1 + n // 4 * 2 + n % 2
        h = n % 4 // 2

        @pl.when(i < NZ)
        def _():
            forward(i, h)
            pack(i, h)

        for at, task in (
            (1, lambda: far_start(2)),
            (3, lambda: far_relay(0)),
            (7, lambda: far_relay(1)),
            (11, lambda: far_relay(2)),
            (12, shared_start),
        ):
            pl.when(n == at)(task)

        @pl.when((n >= 4) & (n != 6) & (n != 8) & (n < 12) & (n != 10))
        def _():
            run_near(jnp.where(n < 6, n - 4, (n - 3) // 2))

        return carry

    shared = ((shg, sg), (shu, su), (shd, sd))

    def twin_half(a, which):
        rows = shared[a][0].shape[0] // NC
        return pl.ds(pl.multiple_of(which * rows, rows), rows)

    def shared_start():
        for copy in local[3:6]:
            copy.wait()
        for dx in (1, 3, 2):
            for a, (mat, full) in enumerate(shared):
                rows = twin_half(a, core)
                send(full.at[0, rows], full.at[dx, rows], x_s.at[a, dx], x_r.at[a, dx], at_x(dx))

    def shared_relay():
        for a, (_, full) in enumerate(shared):
            rows = twin_half(a, core)
            for dx in (1, 3, 2):
                landed(full.at[dx, rows], x_r.at[a, dx])
            send(full.at[others, rows], full.at[others, rows], t_s.at[a], t_r.at[a], twin)

    pack(0, 0)
    pack(0, 1)
    far_start(3)
    far_start(1)
    for copy in local[6:]:
        copy.wait()
    lax.fori_loop(0, 2 * NZ - 1, pieces, 0)

    near_routes = ROUTES[:NEAR]
    run_near(5)
    run_near(6)
    give_back(6, near_routes, (0,))
    run_near(7)
    give_back(7, near_routes)
    give_back(6, near_routes, (1,))
    for a in range(3):
        far_end(a)
    run_far(7)

    def backward(n, carry):
        give_back(5 - n, near_routes)
        return carry

    lax.fori_loop(0, 6, backward, 0)

    def combined(i):
        scaled = placed(i) * inf[i, PLANE : 2 * PLANE, :][:, None, :]
        scaled = jnp.concatenate([scaled.reshape(PACK, ROWS), jnp.zeros((256 - PACK, ROWS), F32)], axis=0)
        scaled = scaled.T[:, :PACK]
        high = scaled.astype(BF)
        low = (scaled - high.astype(F32)).astype(BF)

        def part(h, cols):
            rows = ret[i, h, :, :, cols].reshape(PACK, 512)
            return dot(high, rows) + dot(low, rows)

        return part

    def pass_on(i, h, way):
        send(rst.at[i, h], rsx.at[i, h], p_s.at[i, h], p_r.at[i, h], at_z(way))

    def reduce_piece(i, h, way, source=None):
        part = combined(i)
        landed(ret.at[i, h], e_r.at[i, h])
        if source is not None:
            landed(rsx.at[source, h], p_r.at[source, h])
        for n in range(PART // 512):
            cols = pl.ds(n * 512, 512)
            total = part(h, cols)
            if source is not None:
                total = total + rsx[source, h, :, cols].astype(F32)
            rst[i, h, :, cols] = total.astype(BF)
        pass_on(i, h, way)

    reduce_piece(7, 0, NZ - 1)
    reduce_piece(7, 1, 1)
    run_far(6)
    reduce_piece(6, 0, 1)
    run_far(5)
    reduce_piece(5, 1, NZ - 1)
    reduce_piece(5, 0, NZ - 1, 7)
    reduce_piece(6, 1, 1, 7)

    def nearer(n, carry):
        even, odd = 4 - 2 * n, 3 - 2 * n
        run_far(even)
        reduce_piece(even, 0, 1, even + 2)
        run_far(odd)
        reduce_piece(odd, 1, NZ - 1, odd + 2)
        reduce_piece(even, 1, 1, even + 2)
        reduce_piece(odd, 0, NZ - 1, odd + 2)
        pl.when(n == 1)(shared_relay)
        return carry

    lax.fori_loop(0, 2, nearer, 0)
    run_far(0)

    for a, (_, full) in enumerate(shared):
        landed(full.at[others, twin_half(a, 1 - core)], t_r.at[a])
    sacc[...] = jnp.zeros_like(sacc)

    def shared_block(dx, carry):
        left, right = tok[0, 0], tok[0, 1]
        gate = dot(left, sg[dx, 0:PART]) + dot(right, sg[dx, PART:D])
        up = dot(left, su[dx, 0:PART]) + dot(right, su[dx, PART:D])
        units = (silu(gate) * up).astype(BF)
        for n in range(D // 512):
            cols = pl.ds(n * 512, 512)
            sacc[:, cols] = sacc[:, cols] + dot(units, sd[dx, :, cols])
        return carry

    lax.fori_loop(0, NX, shared_block, 0)

    part = combined(0)
    for h in range(2):
        landed(ret.at[0, h], e_r.at[0, h])
        landed(rsx.at[2, h], p_r.at[2, h])
        landed(rsx.at[1, h], p_r.at[1, h])
        for n in range(PART // 512):
            cols, wide = pl.ds(n * 512, 512), pl.ds(h * PART + n * 512, 512)
            routed = part(h, cols) + rsx[2, h, :, cols].astype(F32) + rsx[1, h, :, cols].astype(F32)
            out[:, wide] = (resid[:, wide].astype(F32) + sacc[:, wide] + routed).astype(BF)

    for i in range(NZ):
        landed(tx.at[i, :, pl.ds(0, PLANE - 2)], d_s.at[i])
        if i > 0:
            landed(info.at[i], i_s.at[i])
        for h in range(2):
            landed(rx.at[i, h, pl.ds(0, PLANE - 2)], e_s.at[i, h])
            if i > 0:
                landed(tok.at[i, h], z_s.at[i, h])
                landed(rst.at[i, h], p_s.at[i, h])
    landed(ekv.at[:, pl.ds(0, WINDOW)], h_s.at[0])
    landed(edoc.at[0], h_s.at[1])
    landed(ekv.at[:, pl.ds(0, WINDOW)], h_s.at[2])
    landed(edoc.at[0], h_s.at[3])
    for dx in range(1, NX):
        landed(atf.at[0], a_s.at[dx])
        landed(wo.at[0, direct], o_s.at[dx])
        landed(wo.at[0, direct], f_s.at[dx])
        for a, (_, full) in enumerate(shared):
            landed(full.at[0, twin_half(a, core)], x_s.at[a, dx])
    for a, (_, full) in enumerate(shared):
        landed(full.at[others, twin_half(a, core)], t_s.at[a])
        landed(far[a].at[eighth(a, 0, 0)], u_s.at[a, 0])
        landed(far[a].at[eighth(a, 0, 0)], u_s.at[a, 2])
    for k in range(4):
        a, rows = unit(k)
        landed(far[a].at[rows], q_s.at[k])
        landed(far[a].at[rows], u_s.at[k, 1])
        landed(far[a].at[rows], u_s.at[k, 3])


def shards(
    queries,
    keys,
    values,
    doc_ids,
    sink_logit,
    w_out,
    residual,
    ffn_gain,
    expert_ids,
    expert_weight,
    exp_gate,
    exp_up,
    exp_down,
    shared_gate,
    shared_up,
    shared_down,
):
    vmem = pl.BlockSpec(memory_space=pltpu.VMEM)
    smem = pl.BlockSpec(memory_space=pltpu.SMEM)
    hbm = pl.BlockSpec(memory_space=pl.ANY)
    dma = pltpu.SemaphoreType.DMA
    unit = FF // NX
    return pl.pallas_call(
        layer_kernel,
        out_shape=jax.ShapeDtypeStruct((ROWS, D), BF),
        in_specs=[hbm, vmem, vmem, vmem, smem, hbm, hbm, vmem, vmem, vmem] + [hbm] * 6,
        out_specs=vmem,
        scratch_shapes=[
            pltpu.VMEM((SPAN, HEADS * HD), BF),
            pltpu.VMEM((2 * HD, SPAN + 2 * WINDOW), BF),
            pltpu.VMEM((BLOCKS + 2, 8, ROWS), F32),
            pltpu.VMEM((BLOCKS, ROWS, HEADS * HD), BF),
            pltpu.VMEM((NX, ROWS, HEADS * HD), BF),
            pltpu.VMEM((NX, OUT_ROWS, D), BF),
            pltpu.VMEM((ROWS, D), BF),
            pltpu.VMEM((NZ, 2, ROWS, PART), BF),
            pltpu.VMEM((NZ, 2, PLANE, SLOTS, PART), BF),
            pltpu.VMEM((NZ, 2, PLANE, SLOTS, PART), BF),
            pltpu.VMEM((NZ, 2, PLANE, SLOTS, PART), BF),
            pltpu.VMEM((NZ, 2, ROWS, PART), BF),
            pltpu.VMEM((NZ, 2, ROWS, PART), BF),
            pltpu.VMEM((NZ, 2 * PLANE, ROWS), F32),
            pltpu.VMEM((NZ, 2 * PLANE, ROWS), F32),
            pltpu.VMEM((D, FF), BF),
            pltpu.VMEM((D, FF), BF),
            pltpu.VMEM((FF, D), BF),
            pltpu.VMEM((D, FF), BF),
            pltpu.VMEM((D, FF), BF),
            pltpu.VMEM((FF, D), BF),
            pltpu.VMEM((NX, D, unit), BF),
            pltpu.VMEM((NX, D, unit), BF),
            pltpu.VMEM((NX, unit, D), BF),
            pltpu.VMEM((ROWS, D), F32),
            pltpu.VMEM((PACK, FF), BF),
        ]
        + [dma((4,))] * 8
        + [dma((NZ, 2))] * 2
        + [dma((NZ,))] * 4
        + [dma((NZ, 2))] * 4
        + [dma((3, NX))] * 2
        + [dma((3,))] * 2
        + [dma((4,))] * 2
        + [dma((4, NX))] * 2
        + [dma((9,))],
        compiler_params=pltpu.CompilerParams(
            collective_id=1, has_side_effects=True, vmem_limit_bytes=62 * 2**20
        ),
        name="layer",
    )(
        queries, keys.T, values.T, doc_ids.reshape(BLOCKS, ROWS), sink_logit, w_out, residual,
        ffn_gain.reshape(1, D), expert_ids.T, expert_weight.T,
        exp_gate, exp_up, exp_down, shared_gate, shared_up, shared_down,
    )


def solution(mesh):
    placed = (
        P("sp", "tp"),
        P("sp", "tp"),
        P("sp", "tp"),
        P("sp"),
        P("tp"),
        P("tp", None),
        P(("sp", "tp"), None),
        P(),
        P(("sp", "tp"), None),
        P(("sp", "tp"), None),
        P("sp", None, None),
        P("sp", None, None),
        P("sp", None, None),
        P(None, "tp"),
        P(None, "tp"),
        P("tp", None),
    )
    return jax.shard_map(
        shards, mesh=mesh, in_specs=placed, out_specs=P(("sp", "tp"), None), check_vma=False
    )
```

```python
import functools

import jax
import jax.numpy as jnp
from jax import lax
from jax.experimental import pallas as pl
from jax.experimental.pallas import tpu as pltpu
from jax.sharding import PartitionSpec as P

HD = 64
WINDOW = 128
NZ, NY, NC, NX = 8, 4, 2, 4
PLANE = NY * NC
SP = NZ * PLANE
SPAN = 512
BLOCKS = SPAN // WINDOW
HEADS = 4
OUT_ROWS = HEADS * HD
OUT_HALF = OUT_ROWS // NC
DIRECT = 80
PART = 1024
ROWS = 128
HALF = 64
CAP = 12
SLOTS = 2 * CAP
PACK = PLANE * SLOTS
D = 2048
FF = 512
EXPERTS = 64
MESH = pl.DeviceIdType.MESH
BF = jnp.bfloat16
F32 = jnp.float32

norm_eps = 1e-06


def dot(a, b):
    return jnp.dot(a, b, preferred_element_type=F32)


def silu(v):
    return v / (1.0 + jnp.exp(-v))


def chunk_of(delta):
    return 0 if delta == 0 else (2 * delta - 1 if delta <= NZ // 2 else 2 * (NZ - delta))


NEAR = 6
ROUTES = tuple((2 * n + turn, step, turn) for n, step in enumerate((0, 1, -1, 0)) for turn in range(NC))


def layer_kernel(
    q, k, v, docs, sink, wout, residual, gain, ids, weight, eg, eu, ed, shg, shu, shd, out,
    qv, ekv, edoc, attn, atf, wo, resid,
    tok, tx, rx, ret, rst, rsx, info, inf, wg, wu, wd, vg, vu, vd, sg, su, sd, sacc, hid,
    h_s, h_r, a_s, a_r, o_s, o_r, f_s, f_r, g_s, g_r, c_s, c_r,
    z_s, z_r, i_s, i_r, d_s, d_r, e_s, e_r, p_s, p_r, x_s, x_r, t_s, t_r, q_s, q_r, u_s, u_r, w_s,
):
    sp, x = lax.axis_index("sp"), lax.axis_index("tp")
    z, mine = sp // PLANE, sp % PLANE
    core = sp % NC
    twin = (sp + 1 - 2 * core, x)

    def at_sp(step):
        return ((sp + step) % SP, x)

    def at_z(dz):
        return ((z + dz) % NZ * PLANE + mine, x)

    def at_plane(j):
        return (z * PLANE + j, x)

    def at_x(dx):
        return (sp, (x + dx) % NX)

    def plane_of(dy, turn):
        return (mine // NC + dy + NY) % NY * NC + (core + turn) % NC

    def send(src, dst, ssem, rsem, device):
        copy = pltpu.make_async_remote_copy(
            src_ref=src, dst_ref=dst, send_sem=ssem, recv_sem=rsem, device_id=device, device_id_type=MESH
        )
        copy.start()

    def landed(ref, sem):
        pltpu.make_async_copy(ref, ref, sem).wait()

    local = [
        pltpu.make_async_copy(q, qv, w_s.at[0]),
        pltpu.make_async_copy(residual, resid, w_s.at[1]),
        pltpu.make_async_copy(wout, wo.at[0], w_s.at[2]),
        pltpu.make_async_copy(shg, sg.at[0], w_s.at[3]),
        pltpu.make_async_copy(shu, su.at[0], w_s.at[4]),
        pltpu.make_async_copy(shd, sd.at[0], w_s.at[5]),
        pltpu.make_async_copy(eg.at[0], wg, w_s.at[6]),
        pltpu.make_async_copy(eu.at[0], wu, w_s.at[7]),
        pltpu.make_async_copy(ed.at[0], wd, w_s.at[8]),
    ]
    for copy in local[:2]:
        copy.start()

    barrier = pltpu.get_barrier_semaphore()
    peers = [at_z(dz) for dz in range(1, NZ)] + [at_x(dx) for dx in range(1, NX)]
    peers += [at_plane((mine + off) % PLANE) for off in range(1, PLANE)]
    peers += [at_sp(1), at_sp(SP - 1)]
    for device in peers:
        pl.semaphore_signal(barrier, inc=1, device_id=device, device_id_type=MESH)

    ekv[0:HD, pl.ds(WINDOW, SPAN)] = k[...]
    ekv[HD : 2 * HD, pl.ds(WINDOW, SPAN)] = v[...]
    for b in range(BLOCKS):
        edoc[b + 1] = jnp.broadcast_to(docs[b : b + 1, :].astype(F32), (8, ROWS))

    far = (vg, vu, vd)

    def quarter(a, step):
        rows = far[a].shape[0] // NX
        return pl.ds(pl.multiple_of((x + step) % NX * rows, rows), rows)

    def eighth(a, step, k):
        rows = far[a].shape[0] // NX
        return pl.ds(pl.multiple_of((x + step) % NX * rows + k * (rows // 2), rows // 2), rows // 2)

    def unit(k):
        return (0 if k == 3 else k, eighth(0, 0, k // 3) if k % 3 == 0 else quarter(k, 0))

    def far_fetch(k):
        a, rows = unit(k)
        send((eg, eu, ed)[a].at[0, rows], far[a].at[rows], q_s.at[k], q_r.at[k], at_plane((mine + PLANE // 2) % PLANE))

    def far_start(k):
        a, rows = unit(k)
        own = far[a].at[rows]
        landed(own, q_r.at[k])
        send(own, own, u_s.at[k, 1], u_r.at[k, 1], at_x(1))
        send(own, own, u_s.at[k, 3], u_r.at[k, 3], at_x(3))

    def far_relay(a):
        if a == 0:
            landed(far[0].at[eighth(0, 3, 0)], u_r.at[0, 1])
            landed(far[0].at[eighth(0, 3, 1)], u_r.at[3, 1])
        else:
            landed(far[a].at[quarter(a, 3)], u_r.at[a, 1])
        half = far[a].at[eighth(a, 3, 0)]
        send(half, half, u_s.at[a, 0], u_r.at[a, 0], at_x(1))
        if a == 0:
            landed(far[0].at[eighth(0, 1, 0)], u_r.at[0, 3])
            landed(far[0].at[eighth(0, 1, 1)], u_r.at[3, 3])
        else:
            landed(far[a].at[quarter(a, 1)], u_r.at[a, 3])
        half = far[a].at[eighth(a, 1, 1)]
        send(half, half, u_s.at[a, 2], u_r.at[a, 2], at_x(3))

    def far_end(a):
        landed(far[a].at[eighth(a, 2, 0)], u_r.at[a, 0])
        landed(far[a].at[eighth(a, 2, 1)], u_r.at[a, 2])

    pl.semaphore_wait(barrier, len(peers))
    send(ekv.at[:, pl.ds(WINDOW, WINDOW)], ekv.at[:, pl.ds(WINDOW + SPAN, WINDOW)], h_s.at[0], h_r.at[0], at_sp(SP - 1))
    send(edoc.at[1], edoc.at[BLOCKS + 1], h_s.at[1], h_r.at[1], at_sp(SP - 1))
    send(ekv.at[:, pl.ds(SPAN, WINDOW)], ekv.at[:, pl.ds(0, WINDOW)], h_s.at[2], h_r.at[2], at_sp(1))
    send(edoc.at[BLOCKS], edoc.at[0], h_s.at[3], h_r.at[3], at_sp(1))
    def out_rows(which, start, size):
        return pl.ds(pl.multiple_of(which * OUT_HALF + start, 16), size)

    def share_cols(dz):
        return pl.ds(pl.multiple_of((z + dz) % NZ * (D // NZ), D // NZ), D // NZ)

    direct, spread = out_rows(core, 0, DIRECT), out_rows(core, DIRECT, OUT_HALF - DIRECT)
    rest, rest_spread = out_rows(1 - core, 0, DIRECT), out_rows(1 - core, DIRECT, OUT_HALF - DIRECT)
    others = pl.ds(1, NX - 1)
    for dx in (1, 3, 2):
        send(wout.at[spread, share_cols(0)], wo.at[dx, spread, share_cols(0)], g_s.at[dx], g_r.at[dx], at_x(dx))
    for dx in (1, 3, 2):
        send(wout.at[direct], wo.at[dx, direct], o_s.at[dx], o_r.at[dx], at_x(dx))

    expert = lax.broadcasted_iota(jnp.int32, (EXPERTS, ROWS), 0)
    hits = jnp.zeros((EXPERTS, ROWS), F32)
    wide = jnp.zeros((EXPERTS, ROWS), F32)
    for k in range(ids.shape[0]):
        named = ids[k : k + 1, :] == expert
        hits = hits + named.astype(F32)
        wide = wide + jnp.where(named, weight[k : k + 1, :], 0.0)
    row = lax.broadcasted_iota(jnp.int32, (ROWS, ROWS), 0)
    col = lax.broadcasted_iota(jnp.int32, (ROWS, ROWS), 1)
    earlier = ((row < col) & (row // HALF == col // HALF)).astype(BF)
    rank = dot(hits.astype(BF), earlier)
    half = lax.broadcasted_iota(jnp.int32, (EXPERTS, ROWS), 1) // HALF
    place = jnp.where(hits > 0.0, rank + (half * CAP).astype(F32), -1.0)
    for plane in range(NZ):
        lower = plane * PLANE
        info[plane, 0:PLANE, :] = place[lower : lower + PLANE]
        info[plane, PLANE : 2 * PLANE, :] = wide[lower : lower + PLANE]
    inf[0] = info[z]

    def attention(n, carry):
        b = jnp.where(n < 3, (n + 1) % 3, 3)

        @pl.when(n == 2)
        def _():
            landed(ekv.at[:, pl.ds(WINDOW + SPAN, WINDOW)], h_r.at[0])
            landed(edoc.at[BLOCKS + 1], h_r.at[1])
            landed(ekv.at[:, pl.ds(0, WINDOW)], h_r.at[2])
            landed(edoc.at[0], h_r.at[3])
            for k in (0, 3, 1, 2):
                far_fetch(k)
            for dx in (1, 3, 2):
                landed(wo.at[dx, spread, share_cols(0)], g_r.at[dx])
            mine_of = wo.at[others, spread, share_cols(0)]
            for dz in range(1, NZ):
                send(mine_of, mine_of, c_s.at[dz], c_r.at[dz], at_z(dz))

            @pl.when(sp == 0)
            def _():
                edoc[0] = jnp.full((8, ROWS), -1.0, F32)

            @pl.when(sp == SP - 1)
            def _():
                edoc[BLOCKS + 1] = jnp.full((8, ROWS), -1.0, F32)

        rows = pl.ds(pl.multiple_of(b * WINDOW, WINDOW), WINDOW)
        band = ekv[:, pl.ds(pl.multiple_of(b * WINDOW, WINDOW), 3 * WINDOW)]
        own_doc = jnp.broadcast_to(edoc[b + 1][0:1, :], (WINDOW, WINDOW)).T
        at_row = lax.broadcasted_iota(jnp.int32, (WINDOW, WINDOW), 0)
        at_col = lax.broadcasted_iota(jnp.int32, (WINDOW, WINDOW), 1)
        near = (at_col >= at_row, at_row >= 0, at_col <= at_row)
        allowed = jnp.concatenate(
            [
                ((own_doc == edoc[b + t][0:1, :]) & near[t]).astype(F32)
                for t in range(3)
            ],
            axis=1,
        )
        heads = []
        for h in range(HEADS):
            query = qv[rows, h * HD : (h + 1) * HD]
            scores = dot(query, band[:HD]) * HD ** (-0.5)
            scores = jnp.where(allowed > 0.0, scores, -jnp.inf)
            row_max = jnp.maximum(jnp.max(scores, axis=1, keepdims=True), sink[h])
            grown = jnp.exp(scores - row_max)
            total = jnp.sum(grown, axis=1, keepdims=True) + jnp.exp(sink[h] - row_max)
            probs = (grown / total).astype(BF)
            mixed = lax.dot_general(probs, band[HD:], (((1,), (1,)), ((), ())), preferred_element_type=F32)
            heads.append(mixed.astype(BF))
        attn[b] = jnp.concatenate(heads, axis=1)
        slot = (b + NX - x) % NX

        @pl.when(b != x)
        def _():
            send(attn.at[b], atf.at[slot], a_s.at[slot], a_r.at[slot], (sp, b))

        @pl.when(b == x)
        def _():
            pltpu.make_async_copy(attn.at[b], atf.at[0], a_r.at[0]).start()

        return carry

    local[0].wait()
    lax.fori_loop(0, BLOCKS, attention, 0)

    for copy in local[2:]:
        copy.start()
    for dx in (1, 3, 2):
        landed(wo.at[dx, direct], o_r.at[dx])
        send(wo.at[dx, direct], wo.at[dx, direct], f_s.at[dx], f_r.at[dx], twin)
    for dz in range(1, NZ):
        landed(wo.at[others, spread, share_cols(NZ - dz)], c_r.at[dz])
    send(wo.at[others, spread], wo.at[others, spread], f_s.at[0], f_r.at[0], twin)
    local[1].wait()
    local[2].wait()
    for dx in range(NX):
        landed(atf.at[dx], a_r.at[dx])
    for dx in range(1, NX):
        landed(wo.at[dx, rest], f_r.at[dx])
    landed(wo.at[others, rest_spread], f_r.at[0])

    far_start(0)

    def project(n, squares):
        cols = pl.ds(pl.multiple_of(n * 256, 256), 256)
        mixed = dot(atf[0], wo[0, :, cols])
        for dx in range(1, NX):
            mixed = mixed + dot(atf[dx], wo[dx, :, cols])
        rounded = (resid[:, cols].astype(F32) + mixed).astype(BF)
        resid[:, cols] = rounded
        squared = rounded.astype(F32)
        squared = squared * squared
        return squares + squared[:, :128] + squared[:, 128:]

    squares = lax.fori_loop(0, D // 256, project, jnp.zeros((ROWS, 128), F32))
    scale = lax.rsqrt(jnp.sum(squares, axis=1, keepdims=True) * (1.0 / D) + norm_eps)
    for h in range(2):
        cols = pl.ds(h * PART, PART)
        tok[0, h] = (resid[:, cols].astype(F32) * scale * gain[:, cols]).astype(BF)

    for delta in range(1, NZ):
        i = chunk_of(delta)
        send(info.at[(z + delta) % NZ], inf.at[i], i_s.at[i], i_r.at[i], at_z(delta))
    for h in range(2):
        send(tok.at[0, h], tok.at[1, h], z_s.at[1, h], z_r.at[1, h], at_z(1))
        send(tok.at[0, h], tok.at[2, h], z_s.at[2, h], z_r.at[2, h], at_z(NZ - 1))

    def placed(i):
        slot = lax.broadcasted_iota(jnp.int32, (PLANE, SLOTS, ROWS), 1).astype(F32)
        return (inf[i, 0:PLANE, :][:, None, :] == slot).astype(F32)

    def forward(i, h):
        landed(tok.at[i, h], z_r.at[i, h])

        @pl.when(h == 0)
        def _():
            landed(inf.at[i], i_r.at[i])

        @pl.when((i < 5) | ((i == 5) & (h == 0)) | ((i == 6) & (h == 1)))
        def _():
            way = 1 + (NZ - 2) * ((i + 1) % 2)
            to = jnp.minimum(i + 2, NZ - 1)
            send(tok.at[i, h], tok.at[to, h], z_s.at[to, h], z_r.at[to, h], at_z(way))

    def pack(i, h):
        pick = placed(i).reshape(PACK, ROWS).astype(BF)
        for n in range(PART // 512):
            cols = pl.ds(n * 512, 512)
            tx[i, h, :, :, cols] = dot(pick, tok[i, h, :, cols]).astype(BF).reshape(PLANE, SLOTS, 512)
        for slot, step, turn in ROUTES:
            runner = plane_of(-step, turn)
            expert = plane_of(2, turn) if slot >= NEAR else runner
            if step == 0 and turn == 0:
                pltpu.make_async_copy(tx.at[i, h, expert], rx.at[i, h, slot], d_r.at[i]).start()
            else:
                send(tx.at[i, h, expert], rx.at[i, h, slot], d_s.at[i], d_r.at[i], at_plane(runner))

    def run_expert(i, lower, count, gate_w, up_w, down_w):
        rows, slots = count * SLOTS, pl.ds(lower, count)

        def hidden_tile(n, carry):
            cols = pl.ds(pl.multiple_of(n * 256, 256), 256)
            left, right = rx[i, 0, slots].reshape(rows, PART), rx[i, 1, slots].reshape(rows, PART)
            gate = dot(left, gate_w[0:PART, cols]) + dot(right, gate_w[PART:D, cols])
            up = dot(left, up_w[0:PART, cols]) + dot(right, up_w[PART:D, cols])
            hid[0:rows, cols] = (silu(gate) * up).astype(BF)
            return carry

        lax.fori_loop(0, FF // 256, hidden_tile, 0)

        def out_tile(n, carry):
            cols = pl.ds(pl.multiple_of(n * 512, 512), 512)
            made = dot(hid[0:rows, :], down_w[:, cols]).astype(BF).reshape(count, SLOTS, 512)
            rx[i, n // 2, slots, :, pl.ds(pl.multiple_of(n % 2 * 512, 512), 512)] = made
            return carry

        lax.fori_loop(0, D // 512, out_tile, 0)

    def give_back(i, routes, halves=(0, 1)):
        for h in halves:
            for slot, step, turn in routes:
                source = plane_of(step, turn)
                expert = plane_of(2, 0) if slot >= NEAR else mine
                if step == 0 and turn == 0:
                    pltpu.make_async_copy(rx.at[i, h, slot], ret.at[i, h, expert], e_r.at[i, h]).start()
                else:
                    send(rx.at[i, h, slot], ret.at[i, h, expert], e_s.at[i, h], e_r.at[i, h], at_plane(source))

    def run_near(i):
        landed(rx.at[i], d_r.at[i])
        run_expert(i, 0, NEAR, wg, wu, wd)

    def run_far(i):
        run_expert(i, NEAR, PLANE - NEAR, vg, vu, vd)
        give_back(i, ROUTES[NEAR:])

    def pieces(n, carry):
        i = 1 + n // 4 * 2 + n % 2
        h = n % 4 // 2

        @pl.when(i < NZ)
        def _():
            forward(i, h)
            pack(i, h)

        for at, task in (
            (1, lambda: far_start(1)),
            (3, lambda: far_relay(0)),
            (5, lambda: far_start(2)),
            (8, lambda: far_relay(1)),
            (12, lambda: far_relay(2)),
            (12, shared_start),
        ):
            pl.when(n == at)(task)

        @pl.when((n == 6) | (n == 8) | (n == 10) | (n == 11))
        def _():
            run_near(jnp.where(n == 11, 3, (n - 6) // 2))

        return carry

    shared = ((shg, sg), (shu, su), (shd, sd))

    def twin_half(a, which):
        rows = shared[a][0].shape[0] // NC
        return pl.ds(pl.multiple_of(which * rows, rows), rows)

    def shared_start():
        for copy in local[3:6]:
            copy.wait()
        for dx in (1, 3, 2):
            for a, (mat, full) in enumerate(shared):
                rows = twin_half(a, core)
                send(full.at[0, rows], full.at[dx, rows], x_s.at[a, dx], x_r.at[a, dx], at_x(dx))

    def shared_relay():
        for a, (_, full) in enumerate(shared):
            rows = twin_half(a, core)
            for dx in (1, 3, 2):
                landed(full.at[dx, rows], x_r.at[a, dx])
            send(full.at[others, rows], full.at[others, rows], t_s.at[a], t_r.at[a], twin)

    pack(0, 0)
    pack(0, 1)
    far_start(3)
    for copy in local[6:]:
        copy.wait()
    lax.fori_loop(0, 2 * NZ - 1, pieces, 0)

    near_routes = ROUTES[:NEAR]
    run_near(4)
    run_near(5)
    run_near(6)
    give_back(6, near_routes, (0,))
    run_near(7)
    give_back(7, near_routes)
    give_back(6, near_routes, (1,))
    for a in range(3):
        far_end(a)
    run_far(7)

    def backward(n, carry):
        give_back(5 - n, near_routes)
        return carry

    lax.fori_loop(0, 6, backward, 0)

    def combined(i):
        scaled = placed(i) * inf[i, PLANE : 2 * PLANE, :][:, None, :]
        scaled = jnp.concatenate([scaled.reshape(PACK, ROWS), jnp.zeros((256 - PACK, ROWS), F32)], axis=0)
        scaled = scaled.T[:, :PACK]
        high = scaled.astype(BF)
        low = (scaled - high.astype(F32)).astype(BF)

        def part(h, cols):
            rows = ret[i, h, :, :, cols].reshape(PACK, 512)
            return dot(high, rows) + dot(low, rows)

        return part

    def pass_on(i, h, way):
        send(rst.at[i, h], rsx.at[i, h], p_s.at[i, h], p_r.at[i, h], at_z(way))

    def reduce_piece(i, h, way, source=None):
        part = combined(i)
        landed(ret.at[i, h], e_r.at[i, h])
        if source is not None:
            landed(rsx.at[source, h], p_r.at[source, h])
        for n in range(PART // 512):
            cols = pl.ds(n * 512, 512)
            total = part(h, cols)
            if source is not None:
                total = total + rsx[source, h, :, cols].astype(F32)
            rst[i, h, :, cols] = total.astype(BF)
        pass_on(i, h, way)

    reduce_piece(7, 0, NZ - 1)
    reduce_piece(7, 1, 1)
    run_far(6)
    reduce_piece(6, 0, 1)
    run_far(5)
    reduce_piece(5, 1, NZ - 1)
    reduce_piece(5, 0, NZ - 1, 7)
    reduce_piece(6, 1, 1, 7)

    def nearer(n, carry):
        even, odd = 4 - 2 * n, 3 - 2 * n
        run_far(even)
        reduce_piece(even, 0, 1, even + 2)
        run_far(odd)
        reduce_piece(odd, 1, NZ - 1, odd + 2)
        reduce_piece(even, 1, 1, even + 2)
        reduce_piece(odd, 0, NZ - 1, odd + 2)
        pl.when(n == 1)(shared_relay)
        return carry

    lax.fori_loop(0, 2, nearer, 0)
    run_far(0)

    for a, (_, full) in enumerate(shared):
        landed(full.at[others, twin_half(a, 1 - core)], t_r.at[a])
    sacc[...] = jnp.zeros_like(sacc)

    def shared_block(dx, carry):
        left, right = tok[0, 0], tok[0, 1]
        gate = dot(left, sg[dx, 0:PART]) + dot(right, sg[dx, PART:D])
        up = dot(left, su[dx, 0:PART]) + dot(right, su[dx, PART:D])
        units = (silu(gate) * up).astype(BF)
        for n in range(D // 512):
            cols = pl.ds(n * 512, 512)
            sacc[:, cols] = sacc[:, cols] + dot(units, sd[dx, :, cols])
        return carry

    lax.fori_loop(0, NX, shared_block, 0)

    part = combined(0)
    for h in range(2):
        landed(ret.at[0, h], e_r.at[0, h])
        landed(rsx.at[2, h], p_r.at[2, h])
        landed(rsx.at[1, h], p_r.at[1, h])
        for n in range(PART // 512):
            cols, wide = pl.ds(n * 512, 512), pl.ds(h * PART + n * 512, 512)
            routed = part(h, cols) + rsx[2, h, :, cols].astype(F32) + rsx[1, h, :, cols].astype(F32)
            out[:, wide] = (resid[:, wide].astype(F32) + sacc[:, wide] + routed).astype(BF)

    for i in range(NZ):
        landed(tx.at[i, :, pl.ds(0, PLANE - 2)], d_s.at[i])
        if i > 0:
            landed(info.at[i], i_s.at[i])
        for h in range(2):
            landed(rx.at[i, h, pl.ds(0, PLANE - 2)], e_s.at[i, h])
            if i > 0:
                landed(tok.at[i, h], z_s.at[i, h])
                landed(rst.at[i, h], p_s.at[i, h])
    landed(ekv.at[:, pl.ds(0, WINDOW)], h_s.at[0])
    landed(edoc.at[0], h_s.at[1])
    landed(ekv.at[:, pl.ds(0, WINDOW)], h_s.at[2])
    landed(edoc.at[0], h_s.at[3])
    for dx in range(1, NX):
        landed(atf.at[0], a_s.at[dx])
        landed(wo.at[0, direct], o_s.at[dx])
        landed(wo.at[0, direct], f_s.at[dx])
        landed(wo.at[0, spread, share_cols(0)], g_s.at[dx])
        for a, (_, full) in enumerate(shared):
            landed(full.at[0, twin_half(a, core)], x_s.at[a, dx])
    for a, (_, full) in enumerate(shared):
        landed(full.at[others, twin_half(a, core)], t_s.at[a])
        landed(far[a].at[eighth(a, 0, 0)], u_s.at[a, 0])
        landed(far[a].at[eighth(a, 0, 0)], u_s.at[a, 2])
    landed(wo.at[others, spread], f_s.at[0])
    for dz in range(1, NZ):
        landed(wo.at[others, spread, share_cols(0)], c_s.at[dz])
    for k in range(4):
        a, rows = unit(k)
        landed(far[a].at[rows], q_s.at[k])
        landed(far[a].at[rows], u_s.at[k, 1])
        landed(far[a].at[rows], u_s.at[k, 3])


def shards(
    queries,
    keys,
    values,
    doc_ids,
    sink_logit,
    w_out,
    residual,
    ffn_gain,
    expert_ids,
    expert_weight,
    exp_gate,
    exp_up,
    exp_down,
    shared_gate,
    shared_up,
    shared_down,
):
    vmem = pl.BlockSpec(memory_space=pltpu.VMEM)
    smem = pl.BlockSpec(memory_space=pltpu.SMEM)
    hbm = pl.BlockSpec(memory_space=pl.ANY)
    dma = pltpu.SemaphoreType.DMA
    unit = FF // NX
    return pl.pallas_call(
        layer_kernel,
        out_shape=jax.ShapeDtypeStruct((ROWS, D), BF),
        in_specs=[hbm, vmem, vmem, vmem, smem, hbm, hbm, vmem, vmem, vmem] + [hbm] * 6,
        out_specs=vmem,
        scratch_shapes=[
            pltpu.VMEM((SPAN, HEADS * HD), BF),
            pltpu.VMEM((2 * HD, SPAN + 2 * WINDOW), BF),
            pltpu.VMEM((BLOCKS + 2, 8, ROWS), F32),
            pltpu.VMEM((BLOCKS, ROWS, HEADS * HD), BF),
            pltpu.VMEM((NX, ROWS, HEADS * HD), BF),
            pltpu.VMEM((NX, OUT_ROWS, D), BF),
            pltpu.VMEM((ROWS, D), BF),
            pltpu.VMEM((NZ, 2, ROWS, PART), BF),
            pltpu.VMEM((NZ, 2, PLANE, SLOTS, PART), BF),
            pltpu.VMEM((NZ, 2, PLANE, SLOTS, PART), BF),
            pltpu.VMEM((NZ, 2, PLANE, SLOTS, PART), BF),
            pltpu.VMEM((NZ, 2, ROWS, PART), BF),
            pltpu.VMEM((NZ, 2, ROWS, PART), BF),
            pltpu.VMEM((NZ, 2 * PLANE, ROWS), F32),
            pltpu.VMEM((NZ, 2 * PLANE, ROWS), F32),
            pltpu.VMEM((D, FF), BF),
            pltpu.VMEM((D, FF), BF),
            pltpu.VMEM((FF, D), BF),
            pltpu.VMEM((D, FF), BF),
            pltpu.VMEM((D, FF), BF),
            pltpu.VMEM((FF, D), BF),
            pltpu.VMEM((NX, D, unit), BF),
            pltpu.VMEM((NX, D, unit), BF),
            pltpu.VMEM((NX, unit, D), BF),
            pltpu.VMEM((ROWS, D), F32),
            pltpu.VMEM((PACK, FF), BF),
        ]
        + [dma((4,))] * 10
        + [dma((NZ,))] * 2
        + [dma((NZ, 2))] * 2
        + [dma((NZ,))] * 4
        + [dma((NZ, 2))] * 4
        + [dma((3, NX))] * 2
        + [dma((3,))] * 2
        + [dma((4,))] * 2
        + [dma((4, NX))] * 2
        + [dma((9,))],
        compiler_params=pltpu.CompilerParams(
            collective_id=1, has_side_effects=True, vmem_limit_bytes=62 * 2**20
        ),
        name="layer",
    )(
        queries, keys.T, values.T, doc_ids.reshape(BLOCKS, ROWS), sink_logit, w_out, residual,
        ffn_gain.reshape(1, D), expert_ids.T, expert_weight.T,
        exp_gate, exp_up, exp_down, shared_gate, shared_up, shared_down,
    )


def solution(mesh):
    placed = (
        P("sp", "tp"),
        P("sp", "tp"),
        P("sp", "tp"),
        P("sp"),
        P("tp"),
        P("tp", None),
        P(("sp", "tp"), None),
        P(),
        P(("sp", "tp"), None),
        P(("sp", "tp"), None),
        P("sp", None, None),
        P("sp", None, None),
        P("sp", None, None),
        P(None, "tp"),
        P(None, "tp"),
        P("tp", None),
    )
    return jax.shard_map(
        shards, mesh=mesh, in_specs=placed, out_specs=P(("sp", "tp"), None), check_vma=False
    )
```
